32 devices in a mesh: rep: 2 (over x), fs: 8 (over z, y), tp: 2 (over core).
Axes of the slice: x: 2, y: 2, z: 4, core: 2. Of those that a mesh axis runs over, the one named last changes fastest.
Arguments:
- tokens: bfloat16 [4096, 2048], P(('rep', 'fs'), 'tp'), may hold values from -30 to 30
- first_gain: float32 [2048], replicated, may hold values from 0.1 to 1.9
- up_weight: bfloat16 [2048, 1024], P('fs', 'tp'), may hold values from -0.125 to 0.125
- value_weight: bfloat16 [2048, 1024], P('fs', 'tp'), may hold values from -1 to 1
- value_gain: float32 [1024], P('tp'), may hold values from 0.1 to 1.9
- mix_weight: bfloat16 [8, 128, 128], P('tp'), may hold values from -0.5 to 0.5
- mix_bias: float32 [8, 128], P('tp'), may hold values from 0.1 to 1.9
- back_weight: bfloat16 [1024, 2048], P('fs', 'tp'), may hold values from -0.1875 to 0.1875
- mid_gain: float32 [2048], replicated, may hold values from 0.1 to 1.9
- hidden_weight: bfloat16 [2048, 8192], P('fs', 'tp'), may hold values from -0.125 to 0.125
- down_weight: bfloat16 [8192, 2048], P('tp', 'fs'), may hold values from -0.0625 to 0.0625
- last_gain: float32 [2048], replicated, may hold values from 0.1 to 1.9
Outputs:
- layer_out: bfloat16 [4096, 2048], P(('rep', 'fs'), 'tp')
The draws below stay inside these ranges and needn't reach their ends.
All inputs are finite; a program needn't handle non-finite values.
Results may differ from the reference program's by a relative error of at most 0.015.
Values may be sent and summed in bfloat16 or wider, within the bound.
A program may use at most 128 MiB of HBM per device.

```python
import jax
import jax.numpy as jnp
from jax import lax

D = 2048
GROUPS = 8
GROUP_W = 128
FF = 8192
SEQ = 128
GW = 1024
TOKENS = 4096
COL_DEV = 1024
GW_DEV = 512
N_TP = 2


def block_scales(key, count, reach):
    order = jax.random.permutation(key, count).astype(jnp.float32)
    return jnp.exp(-reach + 2.0 * reach * order / max(count - 1, 1))


def draw_tokens(key, part):
    first, second, third, fourth = jax.random.split(key, 4)
    scales = jnp.repeat(block_scales(first, D // COL_DEV, 1.2), COL_DEV)
    values = jax.random.normal(second, (TOKENS, D), jnp.float32)
    return jnp.clip(values * scales[None, :], -30.0, 30.0).astype(jnp.bfloat16)


def draw_value_weight(key, part):
    first, second = jax.random.split(key)
    scales = jnp.repeat(block_scales(first, GW // GW_DEV, 1.0), GW_DEV)
    base = jax.random.normal(second, (D, GW), jnp.float32)
    values = jnp.clip(base, -6.0, 6.0) * scales[None, :] * D ** (-0.5)
    return jnp.clip(values, -1.0, 1.0).astype(jnp.bfloat16)


def block_levels(own_key, shape, cuts, low, high):
    level = 1.0
    for dim, shards_of in cuts:
        heights = jax.random.uniform(jax.random.fold_in(jax.random.fold_in(own_key, 6), dim), (shards_of,), jnp.float32, low / len(cuts), high / len(cuts))
        level = level * jnp.repeat(jnp.exp(heights), shape[dim] // shards_of).reshape((-1,) + (1,) * (len(shape) - 1 - dim))
    return level


def scatter_about(stream_key, extent, scale, bound, cuts=(), held_as=jnp.bfloat16):
    loudness = block_levels(stream_key, extent, cuts, -0.22, 0.18) if cuts else 1.0
    values = jax.random.normal(stream_key, extent, jnp.float32) * scale * loudness
    return jnp.minimum(jnp.maximum(values, -bound), bound).astype(held_as)


def setup_inputs(seed: int = 0) -> dict:
    splits = jax.random.split(jax.random.key(seed), 13)
    tokens = draw_tokens(jax.random.fold_in(splits[12], 71), 0)
    first_gain = jnp.clip(1.0 + 0.18 * jax.random.normal(splits[1], (D,), jnp.float32), 0.1, 1.9)
    up_weight = scatter_about(splits[2], (D, GW), D ** -0.5, 0.125, ((0, 8), (1, 2)))
    value_weight = draw_value_weight(jax.random.fold_in(splits[12], 71), 0)
    value_gain = jnp.clip(1.0 + 0.18 * jax.random.normal(splits[4], (GW,), jnp.float32), 0.1, 1.9)
    mix_weight = scatter_about(splits[5], (GROUPS, SEQ, SEQ), SEQ ** -0.5, 0.5, ((0, 2),))
    mix_bias = jnp.clip(1.0 + 0.18 * jax.random.normal(splits[6], (GROUPS, SEQ), jnp.float32), 0.1, 1.9)
    back_weight = scatter_about(splits[7], (GW, D), GW ** -0.5, 0.1875, ((0, 8), (1, 2)))
    mid_gain = jnp.clip(1.0 + 0.18 * jax.random.normal(splits[8], (D,), jnp.float32), 0.1, 1.9)
    hidden_weight = scatter_about(splits[9], (D, FF), D ** -0.5, 0.125, ((0, 8), (1, 2)))
    down_weight = scatter_about(splits[10], (FF, D), FF ** -0.5, 0.0625, ((0, 2), (1, 8)))
    last_gain = jnp.clip(1.0 + 0.18 * jax.random.normal(splits[11], (D,), jnp.float32), 0.1, 1.9)
    return {"tokens": tokens, "first_gain": first_gain, "up_weight": up_weight, "value_weight": value_weight, "value_gain": value_gain, "mix_weight": mix_weight, "mix_bias": mix_bias, "back_weight": back_weight, "mid_gain": mid_gain, "hidden_weight": hidden_weight, "down_weight": down_weight, "last_gain": last_gain}


EPS = 1e-06

def scaled(values, gain):
    factor = lax.rsqrt(lax.optimization_barrier(jnp.mean(values * values, axis=-1, keepdims=True)) + EPS)
    return values * factor * gain

def reference(tokens, first_gain, up_weight, value_weight, value_gain, mix_weight, mix_bias, back_weight, mid_gain, hidden_weight, down_weight, last_gain):
    inputs = tokens.astype(jnp.float32)
    normed = scaled(inputs, first_gain).astype(jnp.bfloat16)
    up_part = jax.nn.gelu(jnp.dot(normed, up_weight, preferred_element_type=jnp.float32), approximate=False).astype(jnp.bfloat16)
    value_pre = jax.nn.gelu(jnp.dot(normed, value_weight, preferred_element_type=jnp.float32), approximate=False)
    value_normed = scaled(value_pre, value_gain).astype(jnp.bfloat16)
    causal = jnp.tril(jnp.ones((SEQ, SEQ), dtype=bool))
    masked = jnp.where(causal[None], mix_weight, jnp.zeros_like(mix_weight)).astype(jnp.float32)
    blocks = value_normed.astype(jnp.float32).reshape(TOKENS // SEQ, SEQ, GROUPS, GROUP_W)
    mixed = jnp.einsum('gts,nsgc->ntgc', masked, blocks) + mix_bias.T[None, :, :, None]
    gated = (up_part.astype(jnp.float32) * mixed.reshape(TOKENS, GW)).astype(jnp.bfloat16)
    stream = (inputs + jnp.dot(gated, back_weight, preferred_element_type=jnp.float32)).astype(jnp.bfloat16)
    stream_f = stream.astype(jnp.float32)
    mid_normed = scaled(stream_f, mid_gain).astype(jnp.bfloat16)
    hidden = jnp.square(jax.nn.relu(jnp.dot(mid_normed, hidden_weight, preferred_element_type=jnp.float32))).astype(jnp.bfloat16)
    width = FF // N_TP
    channel_out = jnp.zeros((TOKENS, D), jnp.float32)
    for block in range(N_TP):
        partial_sum = jnp.dot(hidden[:, block * width:(block + 1) * width], down_weight[block * width:(block + 1) * width], preferred_element_type=jnp.float32)
        rounded = lax.optimization_barrier(partial_sum.astype(jnp.bfloat16))
        channel_out = channel_out + rounded.astype(jnp.float32)
    final = stream_f + channel_out
    return scaled(final, last_gain).astype(jnp.bfloat16)
```

```python
import functools

import jax
import jax.numpy as jnp
from jax import lax
from jax.experimental import pallas as pl
from jax.experimental.pallas import tpu as pltpu
from jax.sharding import PartitionSpec as P

EPS = 1e-06
MESH = pl.DeviceIdType.MESH
BF = jnp.bfloat16
F32 = jnp.float32
ALPHA = (
    0.00022905065861350646,
    0.0034082910107109506,
    0.050955695062380861,
    0.18520832239976145,
    1.128379143519084,
)
BETA = (
    -1.1791602954361697e-7,
    0.000023547966471313185,
    0.0010179625278914885,
    0.014070470171167667,
    0.11098505178285362,
    0.49746925110067538,
    1.0,
)


def horner(x, coefs):
    acc = jnp.full_like(x, coefs[0])
    for c in coefs[1:]:
        acc = acc * x + c
    return acc


def gelu(x):
    z = jnp.clip(x * 0.7071067811865476, -3.7439211627767994, 3.7439211627767994)
    z2 = z * z
    return 0.5 * x * (1.0 + z * horner(z2, ALPHA) / horner(z2, BETA))


def kernel(
    dims,
    tok,
    g1,
    up,
    val,
    vg,
    mw,
    mb,
    back,
    g2,
    hid,
    down,
    g3,
    out,
    xbuf,
    nbuf,
    upw,
    vaw,
    bw,
    hw,
    dw,
    vgb,
    mwb,
    mbb,
    upact,
    vact,
    gated,
    sbuf,
    ag,
    part,
    rsr,
    rss,
    ybuf,
    yin,
    tok_s,
    ring_s,
    rlast_s,
    pw_s,
    a2_s,
    x_s,
    hd_s,
    ag_s,
    rs_s,
    y_s,
):
    n, half_rows, cd, span = dims
    dk, gwd = up.shape
    bk = back.shape[0]
    fu = hw.shape[4]
    dcol = down.shape[1]
    width = 2 * cd
    gw = 2 * gwd
    groups = mw.shape[0]
    gc = gwd // groups
    r, f, t = lax.axis_index("rep"), lax.axis_index("fs"), lax.axis_index("tp")
    zn = n // 2
    z, y = f // 2, f % 2
    pos = z * (1 - y) + (n - 1 - z) * y

    def fs_of(p):
        hi = p // zn
        return (2 * p) * (1 - hi) + (2 * (n - 1 - p) + 1) * hi

    def ring(p):
        return lax.rem(p + 2 * n, n)

    partner = (r, f, 1 - t)
    xpeer = (1 - r, f, t)
    nbr = [(r, fs_of(ring(pos + 1)), t), (r, fs_of(ring(pos - 1)), t)]
    sgn = (1, -1)

    def hops(d, c):
        return n // 2 if d == c else n // 2 - 1

    sent = []

    def send(src, dst, sems, dev):
        ss, rs = sems
        cp = pltpu.make_async_remote_copy(
            src_ref=src, dst_ref=dst, send_sem=ss, recv_sem=rs, device_id=dev, device_id_type=MESH
        )
        cp.start()
        sent.append(cp)

    def landed(ref, sems, dev):
        ss, rs = sems
        pltpu.make_async_remote_copy(
            src_ref=ref, dst_ref=ref, send_sem=ss, recv_sem=rs, device_id=dev, device_id_type=MESH
        ).wait_recv()

    barrier = pltpu.get_barrier_semaphore()
    for k in range(1, n):
        pl.semaphore_signal(
            barrier, inc=1, device_id=(r, lax.rem(f + k, n), t), device_id_type=MESH
        )
    pl.semaphore_signal(barrier, inc=1, device_id=partner, device_id_type=MESH)
    pl.semaphore_signal(barrier, inc=1, device_id=xpeer, device_id_type=MESH)
    pl.semaphore_wait(barrier, n + 1)

    def sem2(s, *i):
        return s.at[(0,) + i], s.at[(1,) + i]

    bh = bk // 2

    def slots(q, c, tt):
        fq = fs_of(q)
        w = upw if c == 0 else vaw
        rows = pl.ds(pl.multiple_of(fq * bk + c * bh, bh), bh)
        return w.at[tt, fq], bw.at[tt, rows, :]

    def own(c):
        return (up, val)[c], back.at[pl.ds(c * bh, bh), :]

    def ring_send(s, d, c):
        q = ring(pos - sgn[d] * s)
        dst = slots(q, c, t)
        src = own(c) if s == 0 else dst
        for i in range(2):
            send(src[i], dst[i], sem2(ring_s, d, c, s, i), nbr[d])

    for d in range(2):
        for c in range(2):
            ring_send(0, d, c)

    rows_own = pl.ds(pl.multiple_of(t * half_rows, half_rows), half_rows)
    rows_oth = pl.ds(pl.multiple_of((1 - t) * half_rows, half_rows), half_rows)
    send(tok.at[rows_oth, :], xbuf.at[t], sem2(tok_s, 0), partner)
    send(vg, vgb.at[t], sem2(tok_s, 1), partner)
    send(mw, mwb.at[t], sem2(tok_s, 2), partner)
    send(mb, mbb.at[t], sem2(tok_s, 3), partner)
    for c in range(2):
        dst = slots(pos, c, t)
        src = own(c)
        for i in range(2):
            send(src[i], dst[i], sem2(pw_s, 0, 0, c, i), partner)

    hr, dr = hid.shape[0] // 2, fu // 2

    def hpiece(tt, ff, rr):
        return hw.at[tt, ff, rr]

    def dpiece(tt, ff, rr):
        return dw.at[tt, rr, :, pl.ds(pl.multiple_of(ff * dcol, dcol), dcol)]

    def a2a_send(k):
        g = lax.rem(f + k, n)
        dev = (r, g, t)
        send(
            hid.at[
                pl.ds(pl.multiple_of(r * hr, hr), hr), pl.ds(pl.multiple_of(g * fu, fu), fu)
            ],
            hpiece(t, f, r),
            sem2(a2_s, k, 0),
            dev,
        )
        send(
            down.at[pl.ds(pl.multiple_of(g * fu + r * dr, dr), dr), :],
            dpiece(t, f, r),
            sem2(a2_s, k, 1),
            dev,
        )

    for c in range(2):
        w = (upw, vaw)[c]
        w[t, f] = (up, val)[c][...]
    bw[t, pl.ds(pl.multiple_of(f * bk, bk), bk), :] = back[...]
    own_cols = pl.ds(pl.multiple_of(f * fu, fu), fu)
    for rr in range(2):
        hw[t, f, rr] = hid[rr * hr : (rr + 1) * hr, own_cols]
        dw[t, rr, :, pl.ds(pl.multiple_of(f * dcol, dcol), dcol)] = down[
            pl.ds(pl.multiple_of(f * fu + rr * dr, dr), dr), :
        ]
    xbuf[t] = tok[rows_own, :]
    vgb[t] = vg[...]
    mwb[t] = mw[...]
    mbb[t] = mb[...]

    steps = n // 2
    ks = list(range(1, n))
    for s in range(1, steps):
        for k in ks[: -(-(n - 1) // (steps - 1))]:
            a2a_send(k)
        ks = ks[-(-(n - 1) // (steps - 1)) :]
        for d in range(2):
            for c in range(2):
                q = ring(pos - sgn[d] * s)
                land = slots(q, c, t)
                for i in range(2):
                    landed(land[i], sem2(ring_s, d, c, s - 1, i), nbr[d])
                if s < hops(d, c):
                    ring_send(s, d, c)
                for i in range(2):
                    send(land[i], land[i], sem2(pw_s, s, d, c, i), partner)
        if s == 1:
            for i, ref in enumerate((xbuf.at[1 - t], vgb.at[1 - t], mwb.at[1 - t], mbb.at[1 - t])):
                landed(ref, sem2(tok_s, i), partner)
            xs = [xbuf[i].astype(F32) for i in range(2)]
            tot = sum(jnp.sum(v * v, axis=1, keepdims=True) for v in xs)
            sc = lax.rsqrt(tot / width + EPS)
            for i in range(2):
                cols = slice(i * cd, (i + 1) * cd)
                nbuf[:, cols] = (xs[i] * sc * g1[:, cols]).astype(BF)
    for d in range(2):
        q = ring(pos - sgn[d] * steps)
        land = slots(q, d, t)
        for i in range(2):
            landed(land[i], sem2(ring_s, d, d, steps - 1, i), nbr[d])
            send(land[i], land[i], sem2(pw_s, steps, d, d, i), partner)
    def relay(k):
        g = lax.rem(f - k + n, n)
        hp, dp = hpiece(t, g, r), dpiece(t, g, r)
        for i, p in enumerate((hp, dp)):
            landed(p, sem2(a2_s, k, i), (r, g, t))
            send(p, p, sem2(x_s, k, i), xpeer)
            send(p, p, sem2(hd_s, k, i, 0), partner)

    for c in range(2):
        for i in range(2):
            landed(slots(pos, c, 1 - t)[i], sem2(pw_s, 0, 0, c, i), partner)
    for s in range(1, steps + 1):
        for d in range(2):
            for c in range(2):
                if s <= hops(d, c):
                    q = ring(pos - sgn[d] * s)
                    for i in range(2):
                        landed(slots(q, c, 1 - t)[i], sem2(pw_s, s, d, c, i), partner)
    for rr in range(2):
        send(hpiece(t, f, rr), hpiece(t, f, rr), sem2(hd_s, 0, 0, rr), partner)
        send(dpiece(t, f, rr), dpiece(t, f, rr), sem2(hd_s, 0, 1, rr), partner)
    for k in range(1, n // 2):
        relay(k)

    @pl.loop(0, 2)
    def _(tt):
        a = jnp.dot(nbuf[...], upw[tt].reshape(width, gwd), preferred_element_type=F32)
        upact[tt] = gelu(a).astype(BF)
        b = jnp.dot(nbuf[...], vaw[tt].reshape(width, gwd), preferred_element_type=F32)
        vact[tt] = gelu(b)

    vs = [vact[i] for i in range(2)]
    tot = sum(jnp.sum(v * v, axis=1, keepdims=True) for v in vs)
    vsc = lax.rsqrt(tot / gw + EPS)
    row_i = lax.broadcasted_iota(jnp.int32, (span, span), 0)
    col_i = lax.broadcasted_iota(jnp.int32, (span, span), 1)
    for tt in range(2):
        vn = (vs[tt] * vsc * vgb[tt]).astype(BF)
        for g in range(groups):
            m = mwb[tt, g]
            m = jnp.where(col_i <= row_i, m, jnp.zeros_like(m))
            bias = jnp.broadcast_to(mbb[tt, g : g + 1, :], (span, span))
            bias = jnp.sum(jnp.where(col_i == row_i, bias, 0.0), axis=1, keepdims=True)
            cs = slice(g * gc, (g + 1) * gc)
            for b in range(half_rows // span):
                rs_ = slice(b * span, (b + 1) * span)
                mx = jnp.dot(m, vn[rs_, cs], preferred_element_type=F32) + bias
                gated[rs_, tt * gwd + g * gc : tt * gwd + (g + 1) * gc] = (
                    upact[tt, rs_, cs].astype(F32) * mx
                ).astype(BF)

    @pl.loop(0, 2)
    def _(tt):
        acc = jnp.dot(gated[...], bw[tt], preferred_element_type=F32)
        sbuf[tt] = (xbuf[tt].astype(F32) + acc).astype(BF)

    ss_ = [sbuf[i].astype(F32) for i in range(2)]
    tot = sum(jnp.sum(v * v, axis=1, keepdims=True) for v in ss_)
    sc = lax.rsqrt(tot / width + EPS)
    for i in range(2):
        ag[pos, i] = (ss_[i] * sc * g2[:, i * cd : (i + 1) * cd]).astype(BF)

    def ag_send(s, d, c):
        q = ring(pos - sgn[d] * s)
        send(ag.at[q, c], ag.at[q, c], sem2(ag_s, d, c, s), nbr[d])

    for d in range(2):
        for c in range(2):
            ag_send(0, d, c)

    for k in range(n // 2, n):
        relay(k)
    for k in range(1, n):
        g = lax.rem(f - k + n, n)
        for i, p in enumerate((hpiece(t, g, 1 - r), dpiece(t, g, 1 - r))):
            landed(p, sem2(x_s, k, i), xpeer)
            send(p, p, sem2(hd_s, k, i, 1), partner)
    for rr in range(2):
        landed(hpiece(1 - t, f, rr), sem2(hd_s, 0, 0, rr), partner)
        landed(dpiece(1 - t, f, rr), sem2(hd_s, 0, 1, rr), partner)
    for k in range(1, n):
        g = lax.rem(f - k + n, n)
        for j, rr in enumerate((r, 1 - r)):
            landed(hpiece(1 - t, g, rr), sem2(hd_s, k, 0, j), partner)
            landed(dpiece(1 - t, g, rr), sem2(hd_s, k, 1, j), partner)

    def mixer(q):
        a = jnp.concatenate([ag[q, 0], ag[q, 1]], axis=1)
        hs = []
        for tt in range(2):
            p = jnp.dot(a, hw[tt].reshape(width, fu), preferred_element_type=F32)
            p = jnp.maximum(p, 0.0)
            hs.append((p * p).astype(BF))
        h = jnp.concatenate(hs, axis=1)
        w = dw[...].reshape(2 * fu, width)
        for c in range(2):
            part[q, c] = jnp.dot(h, w[:, c * cd : (c + 1) * cd], preferred_element_type=F32)

    for s in range(1, steps + 1):
        for d in range(2):
            for c in range(2):
                if s <= hops(d, c):
                    q = ring(pos - sgn[d] * s)
                    landed(ag.at[q, c], sem2(ag_s, d, c, s - 1), nbr[d])
                    if s < hops(d, c):
                        ag_send(s, d, c)
        if s == 1:

            @pl.loop(0, 3)
            def _(j):
                mixer(ring(pos + j - 1))
        elif s < steps:

            @pl.loop(0, 2)
            def _(j):
                mixer(ring(pos + s - 2 * s * j))
        else:
            mixer(ring(pos + s))

    for s in range(steps):
        for d in range(2):
            for c in range(2):
                h = hops(d, c)
                if s < h:
                    dest = ring(pos + sgn[d] * (h - s))
                    v = part[dest, c]
                    if s > 0:
                        landed(rsr.at[d, c, s - 1], sem2(rs_s, d, c, s - 1), nbr[d])
                        v = v + rsr[d, c, s - 1].astype(F32)
                    rss[d, c, s] = v.astype(BF)
                    send(rss.at[d, c, s], rsr.at[d, c, s], sem2(rs_s, d, c, s), nbr[d])
    fin = []
    for c in range(2):
        v = part[pos, c]
        for d in range(2):
            h = hops(d, c)
            landed(rsr.at[d, c, h - 1], sem2(rs_s, d, c, h - 1), nbr[d])
            v = v + rsr[d, c, h - 1].astype(F32)
        fin.append(sbuf[c].astype(F32) + v)
    tot = sum(jnp.sum(v * v, axis=1, keepdims=True) for v in fin)
    sc = lax.rsqrt(tot / width + EPS)
    for c in range(2):
        ybuf[c] = (fin[c] * sc * g3[:, c * cd : (c + 1) * cd]).astype(BF)
    send(ybuf.at[1 - t], yin, sem2(y_s, 0), partner)
    out[rows_own, :] = ybuf[t]
    landed(yin, sem2(y_s, 0), partner)
    out[rows_oth, :] = yin[...]
    for cp in sent:
        cp.wait_send()


def fused(mesh, *args):
    tok, g1, up, val, vg, mw, mb, back, g2, hid, down, g3 = args
    n = mesh.shape["fs"]
    rows, cd = tok.shape
    hrows = rows // 2
    span = mw.shape[1]
    dk, gwd = up.shape
    bk = back.shape[0]
    fu = hid.shape[1] // n
    steps = n // 2
    dims = (n, hrows, cd, span)
    v = pltpu.VMEM
    dma = pltpu.SemaphoreType.DMA
    scratch = [
        v((2, hrows, cd), BF),
        v((hrows, 2 * cd), BF),
        v((2, n, dk, gwd), BF),
        v((2, n, dk, gwd), BF),
        v((2, n * bk, cd), BF),
        v((2, n, 2, dk // 2, fu), BF),
        v((2, 2, fu // 2, 2 * cd), BF),
        v((2, 1, gwd), F32),
        v((2,) + mw.shape, BF),
        v((2,) + mb.shape, F32),
        v((2, hrows, gwd), BF),
        v((2, hrows, gwd), F32),
        v((hrows, 2 * gwd), BF),
        v((2, hrows, cd), BF),
        v((n, 2, hrows, cd), BF),
        v((n, 2, hrows, cd), F32),
        v((2, 2, steps, hrows, cd), BF),
        v((2, 2, steps, hrows, cd), BF),
        v((2, hrows, cd), BF),
        v((hrows, cd), BF),
        dma((2, 4)),
        dma((2, 2, 2, steps, 2)),
        dma((1,)),
        dma((2, steps + 1, 2, 2, 2)),
        dma((2, n, 2)),
        dma((2, n, 2)),
        dma((2, n, 2, 2)),
        dma((2, 2, 2, steps)),
        dma((2, 2, 2, steps)),
        dma((2, 1)),
    ]
    return pl.pallas_call(
        functools.partial(kernel, dims),
        out_shape=jax.ShapeDtypeStruct((rows, cd), BF),
        in_specs=[pl.BlockSpec(memory_space=pltpu.VMEM)] * 12,
        out_specs=pl.BlockSpec(memory_space=pltpu.VMEM),
        scratch_shapes=scratch,
        compiler_params=pltpu.CompilerParams(
            collective_id=0, has_side_effects=True, vmem_limit_bytes=62 * 1024 * 1024
        ),
    )(
        tok,
        g1.reshape(1, -1),
        up,
        val,
        vg.reshape(1, -1),
        mw,
        mb,
        back,
        g2.reshape(1, -1),
        hid,
        down,
        g3.reshape(1, -1),
    )


def normalize(values, gain, total, width):
    return values * lax.rsqrt(total / width + EPS) * gain


def on_device(
    tokens,
    first_gain,
    up_weight,
    value_weight,
    value_gain,
    mix_weight,
    mix_bias,
    back_weight,
    mid_gain,
    hidden_weight,
    down_weight,
    last_gain,
):
    col_count = tokens.shape[1]
    row_count = tokens.shape[0]
    width = col_count * lax.axis_size("tp")
    offset = lax.axis_index("tp") * col_count
    inputs = tokens.astype(jnp.float32)
    whole_in = lax.all_gather(tokens, "tp", axis=1, tiled=True).astype(jnp.float32)
    normed = normalize(
        whole_in, first_gain, jnp.sum(whole_in * whole_in, axis=1, keepdims=True), width
    ).astype(jnp.bfloat16)
    gw_dev = up_weight.shape[1]
    block = normed
    up_pre = jnp.dot(
        block,
        lax.all_gather(up_weight, "fs", axis=0, tiled=True),
        preferred_element_type=jnp.float32,
    )
    value_pre = jnp.dot(
        block,
        lax.all_gather(value_weight, "fs", axis=0, tiled=True),
        preferred_element_type=jnp.float32,
    )
    up_part = jax.nn.gelu(up_pre, approximate=False).astype(jnp.bfloat16)
    value_act = jax.nn.gelu(value_pre, approximate=False)
    value_total = lax.psum(jnp.sum(value_act * value_act, axis=1, keepdims=True), "tp")
    value_normed = normalize(
        value_act, value_gain, value_total, gw_dev * lax.axis_size("tp")
    ).astype(jnp.bfloat16)
    group_dev = mix_weight.shape[0]
    span = mix_weight.shape[1]
    causal = jnp.tril(jnp.ones((span, span), dtype=bool))
    masked = jnp.where(causal[None], mix_weight, jnp.zeros_like(mix_weight))
    blocks = value_normed.reshape(row_count // span, span, group_dev, gw_dev // group_dev)
    mixed = (
        jnp.einsum("gts,nsgc->ntgc", masked, blocks, preferred_element_type=jnp.float32)
        + mix_bias.T[None, :, :, None]
    )
    gated = (up_part.astype(jnp.float32) * mixed.reshape(row_count, gw_dev)).astype(jnp.bfloat16)
    gated_all = lax.all_gather(gated, "tp", axis=1, tiled=True)
    block = gated_all
    back = jnp.dot(
        block,
        lax.all_gather(back_weight, "fs", axis=0, tiled=True),
        preferred_element_type=jnp.float32,
    )
    stream = (inputs + back).astype(jnp.bfloat16)
    stream_f = stream.astype(jnp.float32)
    whole_mid = lax.all_gather(stream, "tp", axis=1, tiled=True).astype(jnp.float32)
    mid_normed = normalize(
        whole_mid, mid_gain, jnp.sum(whole_mid * whole_mid, axis=1, keepdims=True), width
    ).astype(jnp.bfloat16)
    block = mid_normed
    hidden_pre = jnp.dot(
        block,
        lax.all_gather(hidden_weight, "fs", axis=0, tiled=True),
        preferred_element_type=jnp.float32,
    )
    hidden = jnp.square(jax.nn.relu(hidden_pre)).astype(jnp.bfloat16)
    partial_terms = jnp.dot(
        hidden,
        lax.all_gather(down_weight, "fs", axis=1, tiled=True),
        preferred_element_type=jnp.float32,
    )
    channel_out = lax.psum_scatter(
        partial_terms.astype(jnp.bfloat16), "tp", scatter_dimension=1, tiled=True
    ).astype(jnp.float32)
    final = stream_f + channel_out
    final_total = lax.psum(jnp.sum(final * final, axis=1, keepdims=True), "tp")
    return normalize(
        final, lax.dynamic_slice_in_dim(last_gain, offset, col_count), final_total, width
    ).astype(jnp.bfloat16)


def fits(mesh, args):
    tok, _, up, _, _, mw, _, back, _, hid, down, _ = args
    n = mesh.shape["fs"]
    rows, cd = tok.shape
    hrows = rows // 2
    fu = hid.shape[1] // n
    if mesh.shape["rep"] != 2 or mesh.shape["tp"] != 2 or n % 2 or n < 4:
        return False
    if hrows % mw.shape[1] or fu % 256 or down.shape[1] % 128 or back.shape[0] % 32:
        return False
    held = 2 * (up.size * 2 + back.size + hid.size + down.size)
    held += 4 * n * (up.size * 2 + back.size) + 4 * (hid.size + down.size)
    held += n * 2 * hrows * cd * 6 + 8 * n * hrows * cd
    return held < 52 * 2**20


def solution(mesh):
    def on_any(*args):
        return fused(mesh, *args) if fits(mesh, args) else on_device(*args)

    return jax.shard_map(
        on_any,
        mesh=mesh,
        in_specs=(
            P(("rep", "fs"), "tp"),
            P(),
            P("fs", "tp"),
            P("fs", "tp"),
            P("tp"),
            P("tp", None, None),
            P("tp", None),
            P("fs", "tp"),
            P(),
            P("fs", "tp"),
            P("tp", "fs"),
            P(),
        ),
        out_specs=P(("rep", "fs"), "tp"),
        check_vma=False,
    )
```

```python
import functools

import jax
import jax.numpy as jnp
from jax import lax
from jax.experimental import pallas as pl
from jax.experimental.pallas import tpu as pltpu
from jax.sharding import PartitionSpec as P

EPS = 1e-06
MESH = pl.DeviceIdType.MESH
BF = jnp.bfloat16
F32 = jnp.float32
ALPHA = (
    0.00022905065861350646,
    0.0034082910107109506,
    0.050955695062380861,
    0.18520832239976145,
    1.128379143519084,
)
BETA = (
    -1.1791602954361697e-7,
    0.000023547966471313185,
    0.0010179625278914885,
    0.014070470171167667,
    0.11098505178285362,
    0.49746925110067538,
    1.0,
)


def horner(x, coefs):
    acc = jnp.full_like(x, coefs[0])
    for c in coefs[1:]:
        acc = acc * x + c
    return acc


def gelu(x):
    z = jnp.clip(x * 0.7071067811865476, -3.7439211627767994, 3.7439211627767994)
    z2 = z * z
    return 0.5 * x * (1.0 + z * horner(z2, ALPHA) / horner(z2, BETA))


def kernel(
    dims,
    tok,
    g1,
    up,
    val,
    vg,
    mw,
    mb,
    back,
    g2,
    hid,
    down,
    g3,
    out,
    xbuf,
    nbuf,
    upw,
    vaw,
    bw,
    hw,
    dw,
    vgb,
    mwb,
    mbb,
    upacc,
    vact,
    upact,
    gated,
    sbuf,
    ag,
    part,
    rsr,
    rss,
    ybuf,
    yin,
    tok_s,
    ring_s,
    xr_s,
    pw_s,
    px_s,
    a2_s,
    x_s,
    hd_s,
    ag_s,
    rs_s,
    y_s,
):
    n, half_rows, cd, span = dims
    dk, gwd = up.shape
    bk = back.shape[0]
    fu = hw.shape[4]
    dcol = down.shape[1]
    width = 2 * cd
    gw = 2 * gwd
    groups = mw.shape[0]
    gc = gwd // groups
    r, f, t = lax.axis_index("rep"), lax.axis_index("fs"), lax.axis_index("tp")
    zn = n // 2
    z, y = f // 2, f % 2
    pos = z * (1 - y) + (n - 1 - z) * y

    def fs_of(p):
        hi = p // zn
        return (2 * p) * (1 - hi) + (2 * (n - 1 - p) + 1) * hi

    def ring(p):
        return lax.rem(p + 2 * n, n)

    partner = (r, f, 1 - t)
    xpeer = (1 - r, f, t)
    nbr = [(r, fs_of(ring(pos + 1)), t), (r, fs_of(ring(pos - 1)), t)]
    sgn = (1, -1)

    def hops(d, c):
        return n // 2 if d == c else n // 2 - 1

    sent = []

    def send(src, dst, sems, dev):
        ss, rs = sems
        cp = pltpu.make_async_remote_copy(
            src_ref=src, dst_ref=dst, send_sem=ss, recv_sem=rs, device_id=dev, device_id_type=MESH
        )
        cp.start()
        sent.append(cp)

    def landed(ref, sems, dev):
        ss, rs = sems
        pltpu.make_async_remote_copy(
            src_ref=ref, dst_ref=ref, send_sem=ss, recv_sem=rs, device_id=dev, device_id_type=MESH
        ).wait_recv()

    barrier = pltpu.get_barrier_semaphore()
    for k in range(1, n):
        pl.semaphore_signal(
            barrier, inc=1, device_id=(r, lax.rem(f + k, n), t), device_id_type=MESH
        )
    pl.semaphore_signal(barrier, inc=1, device_id=partner, device_id_type=MESH)
    pl.semaphore_signal(barrier, inc=1, device_id=xpeer, device_id_type=MESH)
    pl.semaphore_wait(barrier, n + 1)

    def sem2(s, *i):
        return s.at[(0,) + i], s.at[(1,) + i]

    bh = bk // 2
    bq = bh // 2
    ub = 5 * dk // 256 * 16
    ul = dk - ub
    chains = [(d, d) for d in range(2)] + [(d, 1 - d) for d in range(2)]

    def ring_rows(q, c, tt):
        fq = fs_of(q)
        w = upw if c == 0 else vaw
        rows = pl.ds(pl.multiple_of(fq * bk + c * bh + r * bq, bq), bq)
        return w.at[tt, fq, pl.ds(pl.multiple_of(r * ub, 16), ul), :], bw.at[tt, rows, :]

    def rep_rows(q, c, tt, rr):
        fq = fs_of(q)
        w = upw if c == 0 else vaw
        rows = pl.ds(pl.multiple_of(fq * bk + c * bh + rr * bq, bq), bq)
        return w.at[tt, fq, pl.ds(pl.multiple_of(rr * ul, 16), ub), :], bw.at[tt, rows, :]

    def own_rows(c):
        return (
            (up, val)[c].at[pl.ds(pl.multiple_of(r * ub, 16), ul), :],
            back.at[pl.ds(pl.multiple_of(c * bh + r * bq, bq), bq), :],
        )

    def ring_send(s, d, c):
        q = ring(pos - sgn[d] * s)
        dst = ring_rows(q, c, t)
        src = own_rows(c) if s == 0 else dst
        for i in range(2):
            send(src[i], dst[i], sem2(ring_s, d, c, s, i), nbr[d])

    for d, c in chains:
        ring_send(0, d, c)

    rows_own = pl.ds(pl.multiple_of(t * half_rows, half_rows), half_rows)
    rows_oth = pl.ds(pl.multiple_of((1 - t) * half_rows, half_rows), half_rows)
    send(tok.at[rows_oth, :], xbuf.at[t], sem2(tok_s, 0), partner)
    send(vg, vgb.at[t], sem2(tok_s, 1), partner)
    send(mw, mwb.at[t], sem2(tok_s, 2), partner)
    send(mb, mbb.at[t], sem2(tok_s, 3), partner)
    own_slots = (
        (up, upw.at[t, f]),
        (val, vaw.at[t, f]),
        (back, bw.at[t, pl.ds(pl.multiple_of(f * bk, bk), bk), :]),
    )
    for i, (src, dst) in enumerate(own_slots):
        send(src, dst, sem2(tok_s, 4 + i), partner)

    hr, dr = hid.shape[0] // 2, fu // 2

    def hpiece(tt, ff, rr):
        return hw.at[tt, ff, rr]

    def dpiece(tt, ff, rr):
        return dw.at[tt, rr, :, pl.ds(pl.multiple_of(ff * dcol, dcol), dcol)]

    def a2a_send(k):
        g = lax.rem(f + k, n)
        dev = (r, g, t)
        send(
            hid.at[
                pl.ds(pl.multiple_of(r * hr, hr), hr), pl.ds(pl.multiple_of(g * fu, fu), fu)
            ],
            hpiece(t, f, r),
            sem2(a2_s, k, 0),
            dev,
        )
        send(
            down.at[pl.ds(pl.multiple_of(g * fu + r * dr, dr), dr), :],
            dpiece(t, f, r),
            sem2(a2_s, k, 1),
            dev,
        )

    for c in range(2):
        w = (upw, vaw)[c]
        w[t, f] = (up, val)[c][...]
    bw[t, pl.ds(pl.multiple_of(f * bk, bk), bk), :] = back[...]
    own_cols = pl.ds(pl.multiple_of(f * fu, fu), fu)
    for rr in range(2):
        hw[t, f, rr] = hid[rr * hr : (rr + 1) * hr, own_cols]
        dw[t, rr, :, pl.ds(pl.multiple_of(f * dcol, dcol), dcol)] = down[
            pl.ds(pl.multiple_of(f * fu + rr * dr, dr), dr), :
        ]
    xbuf[t] = tok[rows_own, :]
    vgb[t] = vg[...]
    mwb[t] = mw[...]
    mbb[t] = mb[...]

    steps = n // 2
    for i, ref in enumerate((xbuf.at[1 - t], vgb.at[1 - t], mwb.at[1 - t], mbb.at[1 - t])):
        landed(ref, sem2(tok_s, i), partner)
    xs = [xbuf[i].astype(F32) for i in range(2)]
    tot = sum(jnp.sum(v * v, axis=1, keepdims=True) for v in xs)
    sc = lax.rsqrt(tot / width + EPS)
    for i in range(2):
        nrm = (xs[i] * sc * g1[:, i * cd : (i + 1) * cd]).astype(BF)
        for b in range(cd // dk):
            nbuf[i * (cd // dk) + b] = nrm[:, b * dk : (b + 1) * dk]
    oth = pl.ds(pl.multiple_of(f * bk, bk), bk)
    for i, ref in enumerate((upw.at[1 - t, f], vaw.at[1 - t, f], bw.at[1 - t, oth, :])):
        landed(ref, sem2(tok_s, 4 + i), partner)

    def multiply(fq, first):
        for tt in range(2):
            for w, acc in ((upw, upacc), (vaw, vact)):
                p = jnp.dot(nbuf[fq], w[tt, fq], preferred_element_type=F32)
                acc[tt] = p if first else acc[tt] + p

    multiply(f, True)

    def complete(s):
        got = [(d, c, ring(pos - sgn[d] * s)) for d, c in chains if s <= hops(d, c)]
        for d, c, q in got:
            for i, p in enumerate(rep_rows(q, c, t, 1 - r)):
                landed(p, sem2(xr_s, s, d, c, i), xpeer)
                send(p, p, sem2(px_s, s, d, c, i), partner)
        for d, c, q in got:
            for i, p in enumerate(ring_rows(q, c, 1 - t)):
                landed(p, sem2(pw_s, s, d, c, i), partner)
            for i, p in enumerate(rep_rows(q, c, 1 - t, 1 - r)):
                landed(p, sem2(px_s, s, d, c, i), partner)
        if s < steps:

            @pl.loop(0, 2)
            def _(j):
                multiply(fs_of(ring(pos + s - 2 * s * j)), False)
        else:
            multiply(fs_of(ring(pos + s)), False)

    ks = list(range(1, n))
    for s in range(1, steps + 1):
        for d, c in chains:
            if s <= hops(d, c):
                q = ring(pos - sgn[d] * s)
                land = ring_rows(q, c, t)
                for i in range(2):
                    landed(land[i], sem2(ring_s, d, c, s - 1, i), nbr[d])
                if s < hops(d, c):
                    ring_send(s, d, c)
                for i, p in enumerate(rep_rows(q, c, t, r)):
                    send(p, p, sem2(xr_s, s, d, c, i), xpeer)
                for i in range(2):
                    send(land[i], land[i], sem2(pw_s, s, d, c, i), partner)
        if s < steps:
            done = (n - 1) * s // (steps - 1)
            while ks and ks[0] <= done:
                a2a_send(ks.pop(0))
        if s > 1:
            complete(s - 1)

    def relay(k):
        g = lax.rem(f - k + n, n)
        hp, dp = hpiece(t, g, r), dpiece(t, g, r)
        for i, p in enumerate((hp, dp)):
            landed(p, sem2(a2_s, k, i), (r, g, t))
            send(p, p, sem2(x_s, k, i), xpeer)
            send(p, p, sem2(hd_s, k, i, 0), partner)

    for rr in range(2):
        send(hpiece(t, f, rr), hpiece(t, f, rr), sem2(hd_s, 0, 0, rr), partner)
        send(dpiece(t, f, rr), dpiece(t, f, rr), sem2(hd_s, 0, 1, rr), partner)
    first_relays = (n - 1) // 2
    mid_relays = n - 2
    for k in range(1, 1 + first_relays):
        relay(k)
    complete(steps)

    @pl.loop(0, 2)
    def _(tt):
        upact[tt] = gelu(upacc[tt]).astype(BF)
        vact[tt] = gelu(vact[tt])

    vs = [vact[i] for i in range(2)]
    tot = sum(jnp.sum(v * v, axis=1, keepdims=True) for v in vs)
    vsc = lax.rsqrt(tot / gw + EPS)
    row_i = lax.broadcasted_iota(jnp.int32, (span, span), 0)
    col_i = lax.broadcasted_iota(jnp.int32, (span, span), 1)
    for tt in range(2):
        vn = (vs[tt] * vsc * vgb[tt]).astype(BF)
        for g in range(groups):
            m = mwb[tt, g]
            m = jnp.where(col_i <= row_i, m, jnp.zeros_like(m))
            bias = jnp.broadcast_to(mbb[tt, g : g + 1, :], (span, span))
            bias = jnp.sum(jnp.where(col_i == row_i, bias, 0.0), axis=1, keepdims=True)
            cs = slice(g * gc, (g + 1) * gc)
            for b in range(half_rows // span):
                rs_ = slice(b * span, (b + 1) * span)
                mx = jnp.dot(m, vn[rs_, cs], preferred_element_type=F32) + bias
                gated[rs_, tt * gwd + g * gc : tt * gwd + (g + 1) * gc] = (
                    upact[tt, rs_, cs].astype(F32) * mx
                ).astype(BF)

    for k in range(1 + first_relays, 1 + mid_relays):
        relay(k)

    @pl.loop(0, 2)
    def _(tt):
        acc = jnp.dot(gated[...], bw[tt], preferred_element_type=F32)
        sbuf[tt] = (xbuf[tt].astype(F32) + acc).astype(BF)

    ss_ = [sbuf[i].astype(F32) for i in range(2)]
    tot = sum(jnp.sum(v * v, axis=1, keepdims=True) for v in ss_)
    sc = lax.rsqrt(tot / width + EPS)
    for i in range(2):
        ag[pos, i] = (ss_[i] * sc * g2[:, i * cd : (i + 1) * cd]).astype(BF)

    def ag_send(s, d, c):
        q = ring(pos - sgn[d] * s)
        send(ag.at[q, c], ag.at[q, c], sem2(ag_s, d, c, s), nbr[d])

    for d, c in chains:
        ag_send(0, d, c)

    for k in range(1 + mid_relays, n):
        relay(k)
    for k in range(1, n):
        g = lax.rem(f - k + n, n)
        for i, p in enumerate((hpiece(t, g, 1 - r), dpiece(t, g, 1 - r))):
            landed(p, sem2(x_s, k, i), xpeer)
            send(p, p, sem2(hd_s, k, i, 1), partner)
    for rr in range(2):
        landed(hpiece(1 - t, f, rr), sem2(hd_s, 0, 0, rr), partner)
        landed(dpiece(1 - t, f, rr), sem2(hd_s, 0, 1, rr), partner)
    for k in range(1, n):
        g = lax.rem(f - k + n, n)
        for j, rr in enumerate((r, 1 - r)):
            landed(hpiece(1 - t, g, rr), sem2(hd_s, k, 0, j), partner)
            landed(dpiece(1 - t, g, rr), sem2(hd_s, k, 1, j), partner)

    def mixer(q):
        a = jnp.concatenate([ag[q, 0], ag[q, 1]], axis=1)
        hs = []
        for tt in range(2):
            p = jnp.dot(a, hw[tt].reshape(width, fu), preferred_element_type=F32)
            p = jnp.maximum(p, 0.0)
            hs.append((p * p).astype(BF))
        h = jnp.concatenate(hs, axis=1)
        w = dw[...].reshape(2 * fu, width)
        for c in range(2):
            part[q, c] = jnp.dot(h, w[:, c * cd : (c + 1) * cd], preferred_element_type=F32)

    def rs_send(s, d, c):
        h = hops(d, c)
        v = part[ring(pos + sgn[d] * (h - s)), c]
        if s > 0:
            landed(rsr.at[d, c, s - 1], sem2(rs_s, d, c, s - 1), nbr[d])
            v = v + rsr[d, c, s - 1].astype(F32)
        rss[d, c, s] = v.astype(BF)
        send(rss.at[d, c, s], rsr.at[d, c, s], sem2(rs_s, d, c, s), nbr[d])

    for s in range(1, steps + 1):
        for d, c in chains:
            if s <= hops(d, c):
                q = ring(pos - sgn[d] * s)
                landed(ag.at[q, c], sem2(ag_s, d, c, s - 1), nbr[d])
                if s < hops(d, c):
                    ag_send(s, d, c)
        if s == 1:

            @pl.loop(0, 3)
            def _(j):
                mixer(ring(pos + j - 1))
        elif s < steps:

            @pl.loop(0, 2)
            def _(j):
                mixer(ring(pos + s - 2 * s * j))
        else:
            mixer(ring(pos + s))
        if s == steps - 1:
            for d in range(2):
                rs_send(0, d, 1 - d)

    for s in range(steps):
        for d in range(2):
            rs_send(s, d, d)
        if s + 1 < steps - 1:
            for d in range(2):
                rs_send(s + 1, d, 1 - d)
    fin = []
    for c in range(2):
        v = part[pos, c]
        for d in range(2):
            h = hops(d, c)
            landed(rsr.at[d, c, h - 1], sem2(rs_s, d, c, h - 1), nbr[d])
            v = v + rsr[d, c, h - 1].astype(F32)
        fin.append(sbuf[c].astype(F32) + v)
    tot = sum(jnp.sum(v * v, axis=1, keepdims=True) for v in fin)
    sc = lax.rsqrt(tot / width + EPS)
    for c in range(2):
        ybuf[c] = (fin[c] * sc * g3[:, c * cd : (c + 1) * cd]).astype(BF)
    send(ybuf.at[1 - t], yin, sem2(y_s, 0), partner)
    out[rows_own, :] = ybuf[t]
    landed(yin, sem2(y_s, 0), partner)
    out[rows_oth, :] = yin[...]
    for cp in sent:
        cp.wait_send()


def fused(mesh, *args):
    tok, g1, up, val, vg, mw, mb, back, g2, hid, down, g3 = args
    n = mesh.shape["fs"]
    rows, cd = tok.shape
    hrows = rows // 2
    span = mw.shape[1]
    dk, gwd = up.shape
    bk = back.shape[0]
    fu = hid.shape[1] // n
    steps = n // 2
    dims = (n, hrows, cd, span)
    v = pltpu.VMEM
    dma = pltpu.SemaphoreType.DMA
    scratch = [
        v((2, hrows, cd), BF),
        v((n, hrows, dk), BF),
        v((2, n, dk, gwd), BF),
        v((2, n, dk, gwd), BF),
        v((2, n * bk, cd), BF),
        v((2, n, 2, dk // 2, fu), BF),
        v((2, 2, fu // 2, 2 * cd), BF),
        v((2, 1, gwd), F32),
        v((2,) + mw.shape, BF),
        v((2,) + mb.shape, F32),
        v((2, hrows, gwd), F32),
        v((2, hrows, gwd), F32),
        v((2, hrows, gwd), BF),
        v((hrows, 2 * gwd), BF),
        v((2, hrows, cd), BF),
        v((n, 2, hrows, cd), BF),
        v((n, 2, hrows, cd), F32),
        v((2, 2, steps, hrows, cd), BF),
        v((2, 2, steps, hrows, cd), BF),
        v((2, hrows, cd), BF),
        v((hrows, cd), BF),
        dma((2, 7)),
        dma((2, 2, 2, steps, 2)),
        dma((2, steps + 1, 2, 2, 2)),
        dma((2, steps + 1, 2, 2, 2)),
        dma((2, steps + 1, 2, 2, 2)),
        dma((2, n, 2)),
        dma((2, n, 2)),
        dma((2, n, 2, 2)),
        dma((2, 2, 2, steps)),
        dma((2, 2, 2, steps)),
        dma((2, 1)),
    ]
    return pl.pallas_call(
        functools.partial(kernel, dims),
        out_shape=jax.ShapeDtypeStruct((rows, cd), BF),
        in_specs=[pl.BlockSpec(memory_space=pltpu.VMEM)] * 12,
        out_specs=pl.BlockSpec(memory_space=pltpu.VMEM),
        scratch_shapes=scratch,
        compiler_params=pltpu.CompilerParams(
            collective_id=0, has_side_effects=True, vmem_limit_bytes=62 * 1024 * 1024
        ),
    )(
        tok,
        g1.reshape(1, -1),
        up,
        val,
        vg.reshape(1, -1),
        mw,
        mb,
        back,
        g2.reshape(1, -1),
        hid,
        down,
        g3.reshape(1, -1),
    )


def normalize(values, gain, total, width):
    return values * lax.rsqrt(total / width + EPS) * gain


def on_device(
    tokens,
    first_gain,
    up_weight,
    value_weight,
    value_gain,
    mix_weight,
    mix_bias,
    back_weight,
    mid_gain,
    hidden_weight,
    down_weight,
    last_gain,
):
    col_count = tokens.shape[1]
    row_count = tokens.shape[0]
    width = col_count * lax.axis_size("tp")
    offset = lax.axis_index("tp") * col_count
    inputs = tokens.astype(jnp.float32)
    whole_in = lax.all_gather(tokens, "tp", axis=1, tiled=True).astype(jnp.float32)
    normed = normalize(
        whole_in, first_gain, jnp.sum(whole_in * whole_in, axis=1, keepdims=True), width
    ).astype(jnp.bfloat16)
    gw_dev = up_weight.shape[1]
    block = normed
    up_pre = jnp.dot(
        block,
        lax.all_gather(up_weight, "fs", axis=0, tiled=True),
        preferred_element_type=jnp.float32,
    )
    value_pre = jnp.dot(
        block,
        lax.all_gather(value_weight, "fs", axis=0, tiled=True),
        preferred_element_type=jnp.float32,
    )
    up_part = jax.nn.gelu(up_pre, approximate=False).astype(jnp.bfloat16)
    value_act = jax.nn.gelu(value_pre, approximate=False)
    value_total = lax.psum(jnp.sum(value_act * value_act, axis=1, keepdims=True), "tp")
    value_normed = normalize(
        value_act, value_gain, value_total, gw_dev * lax.axis_size("tp")
    ).astype(jnp.bfloat16)
    group_dev = mix_weight.shape[0]
    span = mix_weight.shape[1]
    causal = jnp.tril(jnp.ones((span, span), dtype=bool))
    masked = jnp.where(causal[None], mix_weight, jnp.zeros_like(mix_weight))
    blocks = value_normed.reshape(row_count // span, span, group_dev, gw_dev // group_dev)
    mixed = (
        jnp.einsum("gts,nsgc->ntgc", masked, blocks, preferred_element_type=jnp.float32)
        + mix_bias.T[None, :, :, None]
    )
    gated = (up_part.astype(jnp.float32) * mixed.reshape(row_count, gw_dev)).astype(jnp.bfloat16)
    gated_all = lax.all_gather(gated, "tp", axis=1, tiled=True)
    block = gated_all
    back = jnp.dot(
        block,
        lax.all_gather(back_weight, "fs", axis=0, tiled=True),
        preferred_element_type=jnp.float32,
    )
    stream = (inputs + back).astype(jnp.bfloat16)
    stream_f = stream.astype(jnp.float32)
    whole_mid = lax.all_gather(stream, "tp", axis=1, tiled=True).astype(jnp.float32)
    mid_normed = normalize(
        whole_mid, mid_gain, jnp.sum(whole_mid * whole_mid, axis=1, keepdims=True), width
    ).astype(jnp.bfloat16)
    block = mid_normed
    hidden_pre = jnp.dot(
        block,
        lax.all_gather(hidden_weight, "fs", axis=0, tiled=True),
        preferred_element_type=jnp.float32,
    )
    hidden = jnp.square(jax.nn.relu(hidden_pre)).astype(jnp.bfloat16)
    partial_terms = jnp.dot(
        hidden,
        lax.all_gather(down_weight, "fs", axis=1, tiled=True),
        preferred_element_type=jnp.float32,
    )
    channel_out = lax.psum_scatter(
        partial_terms.astype(jnp.bfloat16), "tp", scatter_dimension=1, tiled=True
    ).astype(jnp.float32)
    final = stream_f + channel_out
    final_total = lax.psum(jnp.sum(final * final, axis=1, keepdims=True), "tp")
    return normalize(
        final, lax.dynamic_slice_in_dim(last_gain, offset, col_count), final_total, width
    ).astype(jnp.bfloat16)


def fits(mesh, args):
    tok, _, up, _, _, mw, _, back, _, hid, down, _ = args
    n = mesh.shape["fs"]
    rows, cd = tok.shape
    hrows = rows // 2
    fu = hid.shape[1] // n
    if mesh.shape["rep"] != 2 or mesh.shape["tp"] != 2 or n % 2 or n < 4:
        return False
    if hrows % mw.shape[1] or fu % 256 or down.shape[1] % 128 or up.shape[0] % 256 or back.shape[0] % 64:
        return False
    held = 2 * (up.size * 2 + back.size + hid.size + down.size)
    held += 4 * n * (up.size * 2 + back.size) + 4 * (hid.size + down.size)
    held += n * 2 * hrows * cd * 6 + 8 * n * hrows * cd
    return held < 52 * 2**20


def solution(mesh):
    def on_any(*args):
        return fused(mesh, *args) if fits(mesh, args) else on_device(*args)

    return jax.shard_map(
        on_any,
        mesh=mesh,
        in_specs=(
            P(("rep", "fs"), "tp"),
            P(),
            P("fs", "tp"),
            P("fs", "tp"),
            P("tp"),
            P("tp", None, None),
            P("tp", None),
            P("fs", "tp"),
            P(),
            P("fs", "tp"),
            P("tp", "fs"),
            P(),
        ),
        out_specs=P(("rep", "fs"), "tp"),
        check_vma=False,
    )
```

```python
import functools

import jax
import jax.numpy as jnp
from jax import lax
from jax.experimental import pallas as pl
from jax.experimental.pallas import tpu as pltpu
from jax.sharding import PartitionSpec as P

EPS = 1e-06
MESH = pl.DeviceIdType.MESH
BF = jnp.bfloat16
F32 = jnp.float32
ALPHA = (
    0.00022905065861350646,
    0.0034082910107109506,
    0.050955695062380861,
    0.18520832239976145,
    1.128379143519084,
)
BETA = (
    -1.1791602954361697e-7,
    0.000023547966471313185,
    0.0010179625278914885,
    0.014070470171167667,
    0.11098505178285362,
    0.49746925110067538,
    1.0,
)


def horner(x, coefs):
    acc = jnp.full_like(x, coefs[0])
    for c in coefs[1:]:
        acc = acc * x + c
    return acc


def gelu(x):
    z = jnp.clip(x * 0.7071067811865476, -3.7439211627767994, 3.7439211627767994)
    z2 = z * z
    return 0.5 * x * (1.0 + z * horner(z2, ALPHA) / horner(z2, BETA))


def kernel(
    dims,
    tok,
    g1,
    up,
    val,
    vg,
    mw,
    mb,
    back,
    g2,
    hid,
    down,
    g3,
    out,
    xbuf,
    nbuf,
    upw,
    vaw,
    bw,
    hw,
    dw,
    vgb,
    mwb,
    mbb,
    upacc,
    vact,
    upact,
    gated,
    sbuf,
    ag,
    part,
    rsr,
    rss,
    ybuf,
    yin,
    tok_s,
    ring_s,
    xr_s,
    pw_s,
    px_s,
    a2_s,
    x_s,
    hd_s,
    ag_s,
    rs_s,
    y_s,
):
    n, half_rows, cd, span = dims
    dk, gwd = up.shape
    bk = back.shape[0]
    fu = hw.shape[4]
    dcol = down.shape[1]
    width = 2 * cd
    gw = 2 * gwd
    groups = mw.shape[0]
    gc = gwd // groups
    r, f, t = lax.axis_index("rep"), lax.axis_index("fs"), lax.axis_index("tp")
    zn = n // 2
    z, y = f // 2, f % 2
    pos = z * (1 - y) + (n - 1 - z) * y

    def fs_of(p):
        hi = p // zn
        return (2 * p) * (1 - hi) + (2 * (n - 1 - p) + 1) * hi

    def ring(p):
        return lax.rem(p + 2 * n, n)

    partner = (r, f, 1 - t)
    xpeer = (1 - r, f, t)
    nbr = [(r, fs_of(ring(pos + 1)), t), (r, fs_of(ring(pos - 1)), t)]
    sgn = (1, -1)

    def hops(d, c):
        return n // 2 if d == c else n // 2 - 1

    sent = []

    def send(src, dst, sems, dev):
        ss, rs = sems
        cp = pltpu.make_async_remote_copy(
            src_ref=src, dst_ref=dst, send_sem=ss, recv_sem=rs, device_id=dev, device_id_type=MESH
        )
        cp.start()
        sent.append(cp)

    def landed(ref, sems, dev):
        ss, rs = sems
        pltpu.make_async_remote_copy(
            src_ref=ref, dst_ref=ref, send_sem=ss, recv_sem=rs, device_id=dev, device_id_type=MESH
        ).wait_recv()

    barrier = pltpu.get_barrier_semaphore()
    for k in range(1, n):
        pl.semaphore_signal(
            barrier, inc=1, device_id=(r, lax.rem(f + k, n), t), device_id_type=MESH
        )
    pl.semaphore_signal(barrier, inc=1, device_id=partner, device_id_type=MESH)
    pl.semaphore_signal(barrier, inc=1, device_id=xpeer, device_id_type=MESH)
    pl.semaphore_wait(barrier, n + 1)

    def sem2(s, *i):
        return s.at[(0,) + i], s.at[(1,) + i]

    bh = bk // 2
    bq = bh // 2
    ub = dk // 2
    ul = dk - ub
    chains = [(d, d) for d in range(2)] + [(d, 1 - d) for d in range(2)]

    def ring_rows(q, c, tt):
        fq = fs_of(q)
        w = upw if c == 0 else vaw
        rows = pl.ds(pl.multiple_of(fq * bk + c * bh + r * bq, bq), bq)
        return w.at[tt, fq, pl.ds(pl.multiple_of(r * ub, 16), ul), :], bw.at[tt, rows, :]

    def rep_rows(q, c, tt, rr):
        fq = fs_of(q)
        w = upw if c == 0 else vaw
        rows = pl.ds(pl.multiple_of(fq * bk + c * bh + rr * bq, bq), bq)
        return w.at[tt, fq, pl.ds(pl.multiple_of(rr * ul, 16), ub), :], bw.at[tt, rows, :]

    def own_rows(c):
        return (
            (up, val)[c].at[pl.ds(pl.multiple_of(r * ub, 16), ul), :],
            back.at[pl.ds(pl.multiple_of(c * bh + r * bq, bq), bq), :],
        )

    def ring_send(s, d, c):
        q = ring(pos - sgn[d] * s)
        dst = ring_rows(q, c, t)
        src = own_rows(c) if s == 0 else dst
        for i in range(2):
            send(src[i], dst[i], sem2(ring_s, d, c, s, i), nbr[d])

    for d, c in chains:
        ring_send(0, d, c)

    rows_own = pl.ds(pl.multiple_of(t * half_rows, half_rows), half_rows)
    rows_oth = pl.ds(pl.multiple_of((1 - t) * half_rows, half_rows), half_rows)
    send(tok.at[rows_oth, :], xbuf.at[t], sem2(tok_s, 0), partner)
    send(vg, vgb.at[t], sem2(tok_s, 1), partner)
    send(mw, mwb.at[t], sem2(tok_s, 2), partner)
    send(mb, mbb.at[t], sem2(tok_s, 3), partner)
    own_slots = (
        (up, upw.at[t, f]),
        (val, vaw.at[t, f]),
        (back, bw.at[t, pl.ds(pl.multiple_of(f * bk, bk), bk), :]),
    )
    for i, (src, dst) in enumerate(own_slots):
        send(src, dst, sem2(tok_s, 4 + i), partner)

    hr, dr = hid.shape[0] // 2, fu // 2

    def hpiece(tt, ff, rr):
        return hw.at[tt, ff, rr]

    def dpiece(tt, ff, rr):
        return dw.at[tt, rr, :, pl.ds(pl.multiple_of(ff * dcol, dcol), dcol)]

    def a2a_send(k):
        g = lax.rem(f + k, n)
        dev = (r, g, t)
        send(
            hid.at[
                pl.ds(pl.multiple_of(r * hr, hr), hr), pl.ds(pl.multiple_of(g * fu, fu), fu)
            ],
            hpiece(t, f, r),
            sem2(a2_s, k, 0),
            dev,
        )
        send(
            down.at[pl.ds(pl.multiple_of(g * fu + r * dr, dr), dr), :],
            dpiece(t, f, r),
            sem2(a2_s, k, 1),
            dev,
        )

    for c in range(2):
        w = (upw, vaw)[c]
        w[t, f] = (up, val)[c][...]
    bw[t, pl.ds(pl.multiple_of(f * bk, bk), bk), :] = back[...]
    own_cols = pl.ds(pl.multiple_of(f * fu, fu), fu)
    for rr in range(2):
        hw[t, f, rr] = hid[rr * hr : (rr + 1) * hr, own_cols]
        dw[t, rr, :, pl.ds(pl.multiple_of(f * dcol, dcol), dcol)] = down[
            pl.ds(pl.multiple_of(f * fu + rr * dr, dr), dr), :
        ]
    xbuf[t] = tok[rows_own, :]
    vgb[t] = vg[...]
    mwb[t] = mw[...]
    mbb[t] = mb[...]

    steps = n // 2
    for i, ref in enumerate((xbuf.at[1 - t], vgb.at[1 - t], mwb.at[1 - t], mbb.at[1 - t])):
        landed(ref, sem2(tok_s, i), partner)
    xs = [xbuf[i].astype(F32) for i in range(2)]
    tot = sum(jnp.sum(v * v, axis=1, keepdims=True) for v in xs)
    sc = lax.rsqrt(tot / width + EPS)
    for i in range(2):
        nrm = (xs[i] * sc * g1[:, i * cd : (i + 1) * cd]).astype(BF)
        for b in range(cd // dk):
            nbuf[i * (cd // dk) + b] = nrm[:, b * dk : (b + 1) * dk]
    oth = pl.ds(pl.multiple_of(f * bk, bk), bk)
    for i, ref in enumerate((upw.at[1 - t, f], vaw.at[1 - t, f], bw.at[1 - t, oth, :])):
        landed(ref, sem2(tok_s, 4 + i), partner)

    def multiply(fq, first):
        for tt in range(2):
            for w, acc in ((upw, upacc), (vaw, vact)):
                p = jnp.dot(nbuf[fq], w[tt, fq], preferred_element_type=F32)
                acc[tt] = p if first else acc[tt] + p

    multiply(f, True)

    def complete(s):
        got = [(d, c, ring(pos - sgn[d] * s)) for d, c in chains if s <= hops(d, c)]
        for d, c, q in got:
            for i, p in enumerate(rep_rows(q, c, t, 1 - r)):
                landed(p, sem2(xr_s, s, d, c, i), xpeer)
                send(p, p, sem2(px_s, s, d, c, i), partner)
        for d, c, q in got:
            for i, p in enumerate(ring_rows(q, c, 1 - t)):
                landed(p, sem2(pw_s, s, d, c, i), partner)
            for i, p in enumerate(rep_rows(q, c, 1 - t, 1 - r)):
                landed(p, sem2(px_s, s, d, c, i), partner)
        if s < steps:

            @pl.loop(0, 2)
            def _(j):
                multiply(fs_of(ring(pos + s - 2 * s * j)), False)
        else:
            multiply(fs_of(ring(pos + s)), False)

    ks = list(range(1, n))
    for s in range(1, steps + 1):
        for d, c in chains:
            if s <= hops(d, c):
                q = ring(pos - sgn[d] * s)
                land = ring_rows(q, c, t)
                for i in range(2):
                    landed(land[i], sem2(ring_s, d, c, s - 1, i), nbr[d])
                if s < hops(d, c):
                    ring_send(s, d, c)
                for i, p in enumerate(rep_rows(q, c, t, r)):
                    send(p, p, sem2(xr_s, s, d, c, i), xpeer)
                for i in range(2):
                    send(land[i], land[i], sem2(pw_s, s, d, c, i), partner)
        if s < steps:
            done = (n - 1) * s // (steps - 1)
            while ks and ks[0] <= done:
                a2a_send(ks.pop(0))
        if s > 1:
            complete(s - 1)

    def relay(k):
        g = lax.rem(f - k + n, n)
        hp, dp = hpiece(t, g, r), dpiece(t, g, r)
        for i, p in enumerate((hp, dp)):
            landed(p, sem2(a2_s, k, i), (r, g, t))
            send(p, p, sem2(x_s, k, i), xpeer)
            send(p, p, sem2(hd_s, k, i, 0), partner)

    for rr in range(2):
        send(hpiece(t, f, rr), hpiece(t, f, rr), sem2(hd_s, 0, 0, rr), partner)
        send(dpiece(t, f, rr), dpiece(t, f, rr), sem2(hd_s, 0, 1, rr), partner)
    first_relays = (n - 1) // 2
    for k in range(1, 1 + first_relays):
        relay(k)
    complete(steps)

    @pl.loop(0, 2)
    def _(tt):
        upact[tt] = gelu(upacc[tt]).astype(BF)
        vact[tt] = gelu(vact[tt])

    vs = [vact[i] for i in range(2)]
    tot = sum(jnp.sum(v * v, axis=1, keepdims=True) for v in vs)
    vsc = lax.rsqrt(tot / gw + EPS)
    row_i = lax.broadcasted_iota(jnp.int32, (span, span), 0)
    col_i = lax.broadcasted_iota(jnp.int32, (span, span), 1)
    for tt in range(2):
        vn = (vs[tt] * vsc * vgb[tt]).astype(BF)
        for g in range(groups):
            m = mwb[tt, g]
            m = jnp.where(col_i <= row_i, m, jnp.zeros_like(m))
            bias = jnp.broadcast_to(mbb[tt, g : g + 1, :], (span, span))
            bias = jnp.sum(jnp.where(col_i == row_i, bias, 0.0), axis=1, keepdims=True)
            cs = slice(g * gc, (g + 1) * gc)
            for b in range(half_rows // span):
                rs_ = slice(b * span, (b + 1) * span)
                mx = jnp.dot(m, vn[rs_, cs], preferred_element_type=F32) + bias
                gated[rs_, tt * gwd + g * gc : tt * gwd + (g + 1) * gc] = (
                    upact[tt, rs_, cs].astype(F32) * mx
                ).astype(BF)

    @pl.loop(0, 2)
    def _(tt):
        acc = jnp.dot(gated[...], bw[tt], preferred_element_type=F32)
        sbuf[tt] = (xbuf[tt].astype(F32) + acc).astype(BF)

    ss_ = [sbuf[i].astype(F32) for i in range(2)]
    tot = sum(jnp.sum(v * v, axis=1, keepdims=True) for v in ss_)
    sc = lax.rsqrt(tot / width + EPS)
    for i in range(2):
        ag[pos, i] = (ss_[i] * sc * g2[:, i * cd : (i + 1) * cd]).astype(BF)

    def ag_send(s, d, c):
        q = ring(pos - sgn[d] * s)
        send(ag.at[q, c], ag.at[q, c], sem2(ag_s, d, c, s), nbr[d])

    for d, c in chains:
        ag_send(0, d, c)

    def ag_step(s):
        for d, c in chains:
            if s <= hops(d, c):
                q = ring(pos - sgn[d] * s)
                landed(ag.at[q, c], sem2(ag_s, d, c, s - 1), nbr[d])
                if s < hops(d, c):
                    ag_send(s, d, c)

    for k in range(1 + first_relays, n):
        relay(k)
    for s in range(1, steps - 1):
        ag_step(s)
    for k in range(1, n):
        g = lax.rem(f - k + n, n)
        for i, p in enumerate((hpiece(t, g, 1 - r), dpiece(t, g, 1 - r))):
            landed(p, sem2(x_s, k, i), xpeer)
            send(p, p, sem2(hd_s, k, i, 1), partner)
    for rr in range(2):
        landed(hpiece(1 - t, f, rr), sem2(hd_s, 0, 0, rr), partner)
        landed(dpiece(1 - t, f, rr), sem2(hd_s, 0, 1, rr), partner)
    for k in range(1, n):
        g = lax.rem(f - k + n, n)
        for j, rr in enumerate((r, 1 - r)):
            landed(hpiece(1 - t, g, rr), sem2(hd_s, k, 0, j), partner)
            landed(dpiece(1 - t, g, rr), sem2(hd_s, k, 1, j), partner)

    def mixer(q):
        a = jnp.concatenate([ag[q, 0], ag[q, 1]], axis=1)
        hs = []
        for tt in range(2):
            p = jnp.dot(a, hw[tt].reshape(width, fu), preferred_element_type=F32)
            p = jnp.maximum(p, 0.0)
            hs.append((p * p).astype(BF))
        h = jnp.concatenate(hs, axis=1)
        w = dw[...].reshape(2 * fu, width)
        for c in range(2):
            part[q, c] = jnp.dot(h, w[:, c * cd : (c + 1) * cd], preferred_element_type=F32)

    def rs_send(s, d, c):
        h = hops(d, c)
        v = part[ring(pos + sgn[d] * (h - s)), c]
        if s > 0:
            landed(rsr.at[d, c, s - 1], sem2(rs_s, d, c, s - 1), nbr[d])
            v = v + rsr[d, c, s - 1].astype(F32)
        rss[d, c, s] = v.astype(BF)
        send(rss.at[d, c, s], rsr.at[d, c, s], sem2(rs_s, d, c, s), nbr[d])

    @pl.loop(0, 3)
    def _(j):
        mixer(ring(pos + j - 1))

    ag_step(steps - 1)
    for s in range(2, steps):

        @pl.loop(0, 2)
        def _(j):
            mixer(ring(pos + s - 2 * s * j))

    for d in range(2):
        rs_send(0, d, 1 - d)
    ag_step(steps)
    mixer(ring(pos + steps))

    for s in range(steps):
        for d in range(2):
            rs_send(s, d, d)
        if s + 1 < steps - 1:
            for d in range(2):
                rs_send(s + 1, d, 1 - d)
    fin = []
    for c in range(2):
        v = part[pos, c]
        for d in range(2):
            h = hops(d, c)
            landed(rsr.at[d, c, h - 1], sem2(rs_s, d, c, h - 1), nbr[d])
            v = v + rsr[d, c, h - 1].astype(F32)
        fin.append(sbuf[c].astype(F32) + v)
    tot = sum(jnp.sum(v * v, axis=1, keepdims=True) for v in fin)
    sc = lax.rsqrt(tot / width + EPS)
    for c in range(2):
        ybuf[c] = (fin[c] * sc * g3[:, c * cd : (c + 1) * cd]).astype(BF)
    send(ybuf.at[1 - t], yin, sem2(y_s, 0), partner)
    out[rows_own, :] = ybuf[t]
    landed(yin, sem2(y_s, 0), partner)
    out[rows_oth, :] = yin[...]
    for cp in sent:
        cp.wait_send()


def fused(mesh, *args):
    tok, g1, up, val, vg, mw, mb, back, g2, hid, down, g3 = args
    n = mesh.shape["fs"]
    rows, cd = tok.shape
    hrows = rows // 2
    span = mw.shape[1]
    dk, gwd = up.shape
    bk = back.shape[0]
    fu = hid.shape[1] // n
    steps = n // 2
    dims = (n, hrows, cd, span)
    v = pltpu.VMEM
    dma = pltpu.SemaphoreType.DMA
    scratch = [
        v((2, hrows, cd), BF),
        v((n, hrows, dk), BF),
        v((2, n, dk, gwd), BF),
        v((2, n, dk, gwd), BF),
        v((2, n * bk, cd), BF),
        v((2, n, 2, dk // 2, fu), BF),
        v((2, 2, fu // 2, 2 * cd), BF),
        v((2, 1, gwd), F32),
        v((2,) + mw.shape, BF),
        v((2,) + mb.shape, F32),
        v((2, hrows, gwd), F32),
        v((2, hrows, gwd), F32),
        v((2, hrows, gwd), BF),
        v((hrows, 2 * gwd), BF),
        v((2, hrows, cd), BF),
        v((n, 2, hrows, cd), BF),
        v((n, 2, hrows, cd), F32),
        v((2, 2, steps, hrows, cd), BF),
        v((2, 2, steps, hrows, cd), BF),
        v((2, hrows, cd), BF),
        v((hrows, cd), BF),
        dma((2, 7)),
        dma((2, 2, 2, steps, 2)),
        dma((2, steps + 1, 2, 2, 2)),
        dma((2, steps + 1, 2, 2, 2)),
        dma((2, steps + 1, 2, 2, 2)),
        dma((2, n, 2)),
        dma((2, n, 2)),
        dma((2, n, 2, 2)),
        dma((2, 2, 2, steps)),
        dma((2, 2, 2, steps)),
        dma((2, 1)),
    ]
    return pl.pallas_call(
        functools.partial(kernel, dims),
        out_shape=jax.ShapeDtypeStruct((rows, cd), BF),
        in_specs=[pl.BlockSpec(memory_space=pltpu.VMEM)] * 12,
        out_specs=pl.BlockSpec(memory_space=pltpu.VMEM),
        scratch_shapes=scratch,
        compiler_params=pltpu.CompilerParams(
            collective_id=0, has_side_effects=True, vmem_limit_bytes=62 * 1024 * 1024
        ),
    )(
        tok,
        g1.reshape(1, -1),
        up,
        val,
        vg.reshape(1, -1),
        mw,
        mb,
        back,
        g2.reshape(1, -1),
        hid,
        down,
        g3.reshape(1, -1),
    )


def normalize(values, gain, total, width):
    return values * lax.rsqrt(total / width + EPS) * gain


def on_device(
    tokens,
    first_gain,
    up_weight,
    value_weight,
    value_gain,
    mix_weight,
    mix_bias,
    back_weight,
    mid_gain,
    hidden_weight,
    down_weight,
    last_gain,
):
    col_count = tokens.shape[1]
    row_count = tokens.shape[0]
    width = col_count * lax.axis_size("tp")
    offset = lax.axis_index("tp") * col_count
    inputs = tokens.astype(jnp.float32)
    whole_in = lax.all_gather(tokens, "tp", axis=1, tiled=True).astype(jnp.float32)
    normed = normalize(
        whole_in, first_gain, jnp.sum(whole_in * whole_in, axis=1, keepdims=True), width
    ).astype(jnp.bfloat16)
    gw_dev = up_weight.shape[1]
    block = normed
    up_pre = jnp.dot(
        block,
        lax.all_gather(up_weight, "fs", axis=0, tiled=True),
        preferred_element_type=jnp.float32,
    )
    value_pre = jnp.dot(
        block,
        lax.all_gather(value_weight, "fs", axis=0, tiled=True),
        preferred_element_type=jnp.float32,
    )
    up_part = jax.nn.gelu(up_pre, approximate=False).astype(jnp.bfloat16)
    value_act = jax.nn.gelu(value_pre, approximate=False)
    value_total = lax.psum(jnp.sum(value_act * value_act, axis=1, keepdims=True), "tp")
    value_normed = normalize(
        value_act, value_gain, value_total, gw_dev * lax.axis_size("tp")
    ).astype(jnp.bfloat16)
    group_dev = mix_weight.shape[0]
    span = mix_weight.shape[1]
    causal = jnp.tril(jnp.ones((span, span), dtype=bool))
    masked = jnp.where(causal[None], mix_weight, jnp.zeros_like(mix_weight))
    blocks = value_normed.reshape(row_count // span, span, group_dev, gw_dev // group_dev)
    mixed = (
        jnp.einsum("gts,nsgc->ntgc", masked, blocks, preferred_element_type=jnp.float32)
        + mix_bias.T[None, :, :, None]
    )
    gated = (up_part.astype(jnp.float32) * mixed.reshape(row_count, gw_dev)).astype(jnp.bfloat16)
    gated_all = lax.all_gather(gated, "tp", axis=1, tiled=True)
    block = gated_all
    back = jnp.dot(
        block,
        lax.all_gather(back_weight, "fs", axis=0, tiled=True),
        preferred_element_type=jnp.float32,
    )
    stream = (inputs + back).astype(jnp.bfloat16)
    stream_f = stream.astype(jnp.float32)
    whole_mid = lax.all_gather(stream, "tp", axis=1, tiled=True).astype(jnp.float32)
    mid_normed = normalize(
        whole_mid, mid_gain, jnp.sum(whole_mid * whole_mid, axis=1, keepdims=True), width
    ).astype(jnp.bfloat16)
    block = mid_normed
    hidden_pre = jnp.dot(
        block,
        lax.all_gather(hidden_weight, "fs", axis=0, tiled=True),
        preferred_element_type=jnp.float32,
    )
    hidden = jnp.square(jax.nn.relu(hidden_pre)).astype(jnp.bfloat16)
    partial_terms = jnp.dot(
        hidden,
        lax.all_gather(down_weight, "fs", axis=1, tiled=True),
        preferred_element_type=jnp.float32,
    )
    channel_out = lax.psum_scatter(
        partial_terms.astype(jnp.bfloat16), "tp", scatter_dimension=1, tiled=True
    ).astype(jnp.float32)
    final = stream_f + channel_out
    final_total = lax.psum(jnp.sum(final * final, axis=1, keepdims=True), "tp")
    return normalize(
        final, lax.dynamic_slice_in_dim(last_gain, offset, col_count), final_total, width
    ).astype(jnp.bfloat16)


def fits(mesh, args):
    tok, _, up, _, _, mw, _, back, _, hid, down, _ = args
    n = mesh.shape["fs"]
    rows, cd = tok.shape
    hrows = rows // 2
    fu = hid.shape[1] // n
    if mesh.shape["rep"] != 2 or mesh.shape["tp"] != 2 or n % 2 or n < 4:
        return False
    if hrows % mw.shape[1] or fu % 256 or down.shape[1] % 128 or up.shape[0] % 256 or back.shape[0] % 64:
        return False
    held = 2 * (up.size * 2 + back.size + hid.size + down.size)
    held += 4 * n * (up.size * 2 + back.size) + 4 * (hid.size + down.size)
    held += n * 2 * hrows * cd * 6 + 8 * n * hrows * cd
    return held < 52 * 2**20


def solution(mesh):
    def on_any(*args):
        return fused(mesh, *args) if fits(mesh, args) else on_device(*args)

    return jax.shard_map(
        on_any,
        mesh=mesh,
        in_specs=(
            P(("rep", "fs"), "tp"),
            P(),
            P("fs", "tp"),
            P("fs", "tp"),
            P("tp"),
            P("tp", None, None),
            P("tp", None),
            P("fs", "tp"),
            P(),
            P("fs", "tp"),
            P("tp", "fs"),
            P(),
        ),
        out_specs=P(("rep", "fs"), "tp"),
        check_vma=False,
    )
```

```python
import functools

import jax
import jax.numpy as jnp
from jax import lax
from jax.experimental import pallas as pl
from jax.experimental.pallas import tpu as pltpu
from jax.sharding import PartitionSpec as P

EPS = 1e-06
MESH = pl.DeviceIdType.MESH
BF = jnp.bfloat16
F32 = jnp.float32
ALPHA = (
    0.00022905065861350646,
    0.0034082910107109506,
    0.050955695062380861,
    0.18520832239976145,
    1.128379143519084,
)
BETA = (
    -1.1791602954361697e-7,
    0.000023547966471313185,
    0.0010179625278914885,
    0.014070470171167667,
    0.11098505178285362,
    0.49746925110067538,
    1.0,
)


def horner(x, coefs):
    acc = jnp.full_like(x, coefs[0])
    for c in coefs[1:]:
        acc = acc * x + c
    return acc


def gelu(x):
    z = jnp.clip(x * 0.7071067811865476, -3.7439211627767994, 3.7439211627767994)
    z2 = z * z
    return 0.5 * x * (1.0 + z * horner(z2, ALPHA) / horner(z2, BETA))


def kernel(
    dims,
    tok,
    g1,
    up,
    val,
    vg,
    mw,
    mb,
    back,
    g2,
    hid,
    down,
    g3,
    out,
    xbuf,
    nbuf,
    upw,
    vaw,
    bw,
    hw,
    dw,
    vgb,
    mwb,
    mbb,
    upacc,
    vact,
    upact,
    gated,
    sbuf,
    ag,
    part,
    rsr,
    rss,
    ybuf,
    yin,
    tok_s,
    ring_s,
    xr_s,
    pw_s,
    px_s,
    a2_s,
    x_s,
    hd_s,
    ag_s,
    rs_s,
    y_s,
    own_s,
):
    n, half_rows, cd, span = dims
    dk, gwd = up.shape
    bk = back.shape[0]
    fu = hw.shape[4]
    dcol = down.shape[1]
    width = 2 * cd
    gw = 2 * gwd
    groups = mw.shape[0]
    gc = gwd // groups
    r, f, t = lax.axis_index("rep"), lax.axis_index("fs"), lax.axis_index("tp")
    zn = n // 2
    z, y = f // 2, f % 2
    pos = z * (1 - y) + (n - 1 - z) * y

    def fs_of(p):
        hi = p // zn
        return (2 * p) * (1 - hi) + (2 * (n - 1 - p) + 1) * hi

    def ring(p):
        return lax.rem(p + 2 * n, n)

    partner = (r, f, 1 - t)
    xpeer = (1 - r, f, t)
    nbr = [(r, fs_of(ring(pos + 1)), t), (r, fs_of(ring(pos - 1)), t)]
    sgn = (1, -1)

    def hops(d, c):
        return n // 2 if d == c else n // 2 - 1

    sent = []

    def send(src, dst, sems, dev):
        ss, rs = sems
        cp = pltpu.make_async_remote_copy(
            src_ref=src, dst_ref=dst, send_sem=ss, recv_sem=rs, device_id=dev, device_id_type=MESH
        )
        cp.start()
        sent.append(cp)

    def landed(ref, sems, dev):
        ss, rs = sems
        pltpu.make_async_remote_copy(
            src_ref=ref, dst_ref=ref, send_sem=ss, recv_sem=rs, device_id=dev, device_id_type=MESH
        ).wait_recv()

    barrier = pltpu.get_barrier_semaphore()
    for k in range(1, n):
        pl.semaphore_signal(
            barrier, inc=1, device_id=(r, lax.rem(f + k, n), t), device_id_type=MESH
        )
    pl.semaphore_signal(barrier, inc=1, device_id=partner, device_id_type=MESH)
    pl.semaphore_signal(barrier, inc=1, device_id=xpeer, device_id_type=MESH)
    pl.semaphore_wait(barrier, n + 1)

    def sem2(s, *i):
        return s.at[(0,) + i], s.at[(1,) + i]

    bh = bk // 2
    bq = bh // 2
    ub = dk // 2
    ul = dk - ub
    chains = [(d, d) for d in range(2)] + [(d, 1 - d) for d in range(2)]

    def ring_rows(q, c, tt):
        fq = fs_of(q)
        w = upw if c == 0 else vaw
        rows = pl.ds(pl.multiple_of(fq * bk + c * bh + r * bq, bq), bq)
        return w.at[tt, fq, pl.ds(pl.multiple_of(r * ub, 16), ul), :], bw.at[tt, rows, :]

    def rep_rows(q, c, tt, rr):
        fq = fs_of(q)
        w = upw if c == 0 else vaw
        rows = pl.ds(pl.multiple_of(fq * bk + c * bh + rr * bq, bq), bq)
        return w.at[tt, fq, pl.ds(pl.multiple_of(rr * ul, 16), ub), :], bw.at[tt, rows, :]

    def own_rows(c):
        return (
            (up, val)[c].at[pl.ds(pl.multiple_of(r * ub, 16), ul), :],
            back.at[pl.ds(pl.multiple_of(c * bh + r * bq, bq), bq), :],
        )

    def ring_send(s, d, c):
        q = ring(pos - sgn[d] * s)
        dst = ring_rows(q, c, t)
        src = own_rows(c) if s == 0 else dst
        for i in range(2):
            send(src[i], dst[i], sem2(ring_s, d, c, s, i), nbr[d])

    for d, c in chains:
        ring_send(0, d, c)

    rows_own = pl.ds(pl.multiple_of(t * half_rows, half_rows), half_rows)
    rows_oth = pl.ds(pl.multiple_of((1 - t) * half_rows, half_rows), half_rows)
    send(tok.at[rows_oth, :], xbuf.at[t], sem2(tok_s, 0), partner)
    send(vg, vgb.at[t], sem2(tok_s, 1), partner)
    send(mw, mwb.at[t], sem2(tok_s, 2), partner)
    send(mb, mbb.at[t], sem2(tok_s, 3), partner)
    own_slots = (
        (up, upw.at[t, f]),
        (val, vaw.at[t, f]),
        (back, bw.at[t, pl.ds(pl.multiple_of(f * bk, bk), bk), :]),
    )
    for i, (src, dst) in enumerate(own_slots):
        send(src, dst, sem2(tok_s, 4 + i), partner)

    hr, dr = hid.shape[0] // 2, fu // 2

    def hpiece(tt, ff, rr):
        return hw.at[tt, ff, rr]

    def dpiece(tt, ff, rr):
        return dw.at[tt, rr, :, pl.ds(pl.multiple_of(ff * dcol, dcol), dcol)]

    def a2a_send(k):
        g = lax.rem(f + k, n)
        dev = (r, g, t)
        send(
            hid.at[
                pl.ds(pl.multiple_of(r * hr, hr), hr), pl.ds(pl.multiple_of(g * fu, fu), fu)
            ],
            hpiece(t, f, r),
            sem2(a2_s, k, 0),
            dev,
        )
        send(
            down.at[pl.ds(pl.multiple_of(g * fu + r * dr, dr), dr), :],
            dpiece(t, f, r),
            sem2(a2_s, k, 1),
            dev,
        )

    a2a_send(1)

    for c in range(2):
        w = (upw, vaw)[c]
        w[t, f] = (up, val)[c][...]
    bw[t, pl.ds(pl.multiple_of(f * bk, bk), bk), :] = back[...]
    own_cols = pl.ds(pl.multiple_of(f * fu, fu), fu)
    local = []
    for rr in range(2):
        local.append(
            pltpu.make_async_copy(
                hid.at[pl.ds(rr * hr, hr), own_cols], hpiece(t, f, rr), own_s.at[rr, 0]
            )
        )
        local.append(
            pltpu.make_async_copy(
                down.at[pl.ds(pl.multiple_of(f * fu + rr * dr, dr), dr), :],
                dpiece(t, f, rr),
                own_s.at[rr, 1],
            )
        )
    for cp in local:
        cp.start()
    xbuf[t] = tok[rows_own, :]
    vgb[t] = vg[...]
    mwb[t] = mw[...]
    mbb[t] = mb[...]

    steps = n // 2
    for i, ref in enumerate((xbuf.at[1 - t], vgb.at[1 - t], mwb.at[1 - t], mbb.at[1 - t])):
        landed(ref, sem2(tok_s, i), partner)
    xs = [xbuf[i].astype(F32) for i in range(2)]
    tot = sum(jnp.sum(v * v, axis=1, keepdims=True) for v in xs)
    sc = lax.rsqrt(tot / width + EPS)
    for i in range(2):
        nrm = (xs[i] * sc * g1[:, i * cd : (i + 1) * cd]).astype(BF)
        for b in range(cd // dk):
            nbuf[i * (cd // dk) + b] = nrm[:, b * dk : (b + 1) * dk]
    oth = pl.ds(pl.multiple_of(f * bk, bk), bk)
    for i, ref in enumerate((upw.at[1 - t, f], vaw.at[1 - t, f], bw.at[1 - t, oth, :])):
        landed(ref, sem2(tok_s, 4 + i), partner)

    def multiply(fq, first):
        for tt in range(2):
            for w, acc in ((upw, upacc), (vaw, vact)):
                p = jnp.dot(nbuf[fq], w[tt, fq], preferred_element_type=F32)
                acc[tt] = p if first else acc[tt] + p

    multiply(f, True)

    def complete(s):
        got = [(d, c, ring(pos - sgn[d] * s)) for d, c in chains if s <= hops(d, c)]
        for d, c, q in got:
            for i, p in enumerate(rep_rows(q, c, t, 1 - r)):
                landed(p, sem2(xr_s, s, d, c, i), xpeer)
                send(p, p, sem2(px_s, s, d, c, i), partner)
        for d, c, q in got:
            for i, p in enumerate(ring_rows(q, c, 1 - t)):
                landed(p, sem2(pw_s, s, d, c, i), partner)
            for i, p in enumerate(rep_rows(q, c, 1 - t, 1 - r)):
                landed(p, sem2(px_s, s, d, c, i), partner)
        if s < steps:

            @pl.loop(0, 2)
            def _(j):
                multiply(fs_of(ring(pos + s - 2 * s * j)), False)
        else:
            multiply(fs_of(ring(pos + s)), False)

    ks = list(range(2, n))
    for s in range(1, steps + 1):
        for d, c in chains:
            if s <= hops(d, c):
                q = ring(pos - sgn[d] * s)
                land = ring_rows(q, c, t)
                for i in range(2):
                    landed(land[i], sem2(ring_s, d, c, s - 1, i), nbr[d])
                if s < hops(d, c):
                    ring_send(s, d, c)
                for i, p in enumerate(rep_rows(q, c, t, r)):
                    send(p, p, sem2(xr_s, s, d, c, i), xpeer)
                for i in range(2):
                    send(land[i], land[i], sem2(pw_s, s, d, c, i), partner)
        if s < steps - 1:
            a2a_send(ks.pop(0))
        elif s == steps - 1:
            for k in ks:
                a2a_send(k)
        if s > 2:
            complete(s - 2)

    def relay(k):
        g = lax.rem(f - k + n, n)
        hp, dp = hpiece(t, g, r), dpiece(t, g, r)
        for i, p in enumerate((hp, dp)):
            landed(p, sem2(a2_s, k, i), (r, g, t))
            send(p, p, sem2(x_s, k, i), xpeer)
            send(p, p, sem2(hd_s, k, i, 0), partner)

    for cp in local:
        cp.wait()
    for rr in range(2):
        send(hpiece(t, f, rr), hpiece(t, f, rr), sem2(hd_s, 0, 0, rr), partner)
        send(dpiece(t, f, rr), dpiece(t, f, rr), sem2(hd_s, 0, 1, rr), partner)
    first_relays = (n - 1) // 2
    for k in range(1, 1 + first_relays):
        relay(k)
    complete(steps - 1)
    complete(steps)

    @pl.loop(0, 2)
    def _(tt):
        upact[tt] = gelu(upacc[tt]).astype(BF)
        vact[tt] = gelu(vact[tt])

    vs = [vact[i] for i in range(2)]
    tot = sum(jnp.sum(v * v, axis=1, keepdims=True) for v in vs)
    vsc = lax.rsqrt(tot / gw + EPS)
    row_i = lax.broadcasted_iota(jnp.int32, (span, span), 0)
    col_i = lax.broadcasted_iota(jnp.int32, (span, span), 1)
    for tt in range(2):
        vn = (vs[tt] * vsc * vgb[tt]).astype(BF)
        for g in range(groups):
            m = mwb[tt, g]
            m = jnp.where(col_i <= row_i, m, jnp.zeros_like(m))
            bias = jnp.broadcast_to(mbb[tt, g : g + 1, :], (span, span))
            bias = jnp.sum(jnp.where(col_i == row_i, bias, 0.0), axis=1, keepdims=True)
            cs = slice(g * gc, (g + 1) * gc)
            for b in range(half_rows // span):
                rs_ = slice(b * span, (b + 1) * span)
                mx = jnp.dot(m, vn[rs_, cs], preferred_element_type=F32) + bias
                gated[rs_, tt * gwd + g * gc : tt * gwd + (g + 1) * gc] = (
                    upact[tt, rs_, cs].astype(F32) * mx
                ).astype(BF)

    @pl.loop(0, 2)
    def _(tt):
        acc = jnp.dot(gated[...], bw[tt], preferred_element_type=F32)
        sbuf[tt] = (xbuf[tt].astype(F32) + acc).astype(BF)

    ss_ = [sbuf[i].astype(F32) for i in range(2)]
    tot = sum(jnp.sum(v * v, axis=1, keepdims=True) for v in ss_)
    sc = lax.rsqrt(tot / width + EPS)
    for i in range(2):
        ag[pos, i] = (ss_[i] * sc * g2[:, i * cd : (i + 1) * cd]).astype(BF)

    def ag_send(s, d, c):
        q = ring(pos - sgn[d] * s)
        send(ag.at[q, c], ag.at[q, c], sem2(ag_s, d, c, s), nbr[d])

    for d, c in chains:
        ag_send(0, d, c)

    def ag_step(s):
        for d, c in chains:
            if s <= hops(d, c):
                q = ring(pos - sgn[d] * s)
                landed(ag.at[q, c], sem2(ag_s, d, c, s - 1), nbr[d])
                if s < hops(d, c):
                    ag_send(s, d, c)

    for k in range(1 + first_relays, n):
        relay(k)
    for s in range(1, steps - 1):
        ag_step(s)
    for k in range(1, n):
        g = lax.rem(f - k + n, n)
        for i, p in enumerate((hpiece(t, g, 1 - r), dpiece(t, g, 1 - r))):
            landed(p, sem2(x_s, k, i), xpeer)
            send(p, p, sem2(hd_s, k, i, 1), partner)
    for rr in range(2):
        landed(hpiece(1 - t, f, rr), sem2(hd_s, 0, 0, rr), partner)
        landed(dpiece(1 - t, f, rr), sem2(hd_s, 0, 1, rr), partner)
    for k in range(1, n):
        g = lax.rem(f - k + n, n)
        for j, rr in enumerate((r, 1 - r)):
            landed(hpiece(1 - t, g, rr), sem2(hd_s, k, 0, j), partner)
            landed(dpiece(1 - t, g, rr), sem2(hd_s, k, 1, j), partner)

    def mixer(q):
        a = jnp.concatenate([ag[q, 0], ag[q, 1]], axis=1)
        hs = []
        for tt in range(2):
            p = jnp.dot(a, hw[tt].reshape(width, fu), preferred_element_type=F32)
            p = jnp.maximum(p, 0.0)
            hs.append((p * p).astype(BF))
        h = jnp.concatenate(hs, axis=1)
        w = dw[...].reshape(2 * fu, width)
        for c in range(2):
            part[q, c] = jnp.dot(h, w[:, c * cd : (c + 1) * cd], preferred_element_type=F32)

    def rs_send(s, d, c):
        h = hops(d, c)
        v = part[ring(pos + sgn[d] * (h - s)), c]
        if s > 0:
            landed(rsr.at[d, c, s - 1], sem2(rs_s, d, c, s - 1), nbr[d])
            v = v + rsr[d, c, s - 1].astype(F32)
        rss[d, c, s] = v.astype(BF)
        send(rss.at[d, c, s], rsr.at[d, c, s], sem2(rs_s, d, c, s), nbr[d])

    ag_step(steps - 1)

    def mixer_pair(s):
        @pl.loop(0, 2)
        def _(j):
            mixer(ring(pos + s - 2 * s * j))

    mixer_pair(steps - 1)
    for d in range(2):
        rs_send(0, d, 1 - d)
    ag_step(steps)
    mixer(ring(pos + steps))
    for s in range(steps):
        for d in range(2):
            rs_send(s, d, d)
        if s + 1 < steps:
            if steps - 2 - s > 0:
                mixer_pair(steps - 2 - s)
            else:
                mixer(pos)
        if s + 1 < steps - 1:
            for d in range(2):
                rs_send(s + 1, d, 1 - d)

    fin = []
    for c in range(2):
        v = part[pos, c]
        for d in range(2):
            h = hops(d, c)
            landed(rsr.at[d, c, h - 1], sem2(rs_s, d, c, h - 1), nbr[d])
            v = v + rsr[d, c, h - 1].astype(F32)
        fin.append(sbuf[c].astype(F32) + v)
    tot = sum(jnp.sum(v * v, axis=1, keepdims=True) for v in fin)
    sc = lax.rsqrt(tot / width + EPS)
    for c in range(2):
        ybuf[c] = (fin[c] * sc * g3[:, c * cd : (c + 1) * cd]).astype(BF)
    send(ybuf.at[1 - t], yin, sem2(y_s, 0), partner)
    out[rows_own, :] = ybuf[t]
    landed(yin, sem2(y_s, 0), partner)
    out[rows_oth, :] = yin[...]
    for cp in sent:
        cp.wait_send()


def fused(mesh, *args):
    tok, g1, up, val, vg, mw, mb, back, g2, hid, down, g3 = args
    n = mesh.shape["fs"]
    rows, cd = tok.shape
    hrows = rows // 2
    span = mw.shape[1]
    dk, gwd = up.shape
    bk = back.shape[0]
    fu = hid.shape[1] // n
    steps = n // 2
    dims = (n, hrows, cd, span)
    v = pltpu.VMEM
    dma = pltpu.SemaphoreType.DMA
    scratch = [
        v((2, hrows, cd), BF),
        v((n, hrows, dk), BF),
        v((2, n, dk, gwd), BF),
        v((2, n, dk, gwd), BF),
        v((2, n * bk, cd), BF),
        v((2, n, 2, dk // 2, fu), BF),
        v((2, 2, fu // 2, 2 * cd), BF),
        v((2, 1, gwd), F32),
        v((2,) + mw.shape, BF),
        v((2,) + mb.shape, F32),
        v((2, hrows, gwd), F32),
        v((2, hrows, gwd), F32),
        v((2, hrows, gwd), BF),
        v((hrows, 2 * gwd), BF),
        v((2, hrows, cd), BF),
        v((n, 2, hrows, cd), BF),
        v((n, 2, hrows, cd), F32),
        v((2, 2, steps, hrows, cd), BF),
        v((2, 2, steps, hrows, cd), BF),
        v((2, hrows, cd), BF),
        v((hrows, cd), BF),
        dma((2, 7)),
        dma((2, 2, 2, steps, 2)),
        dma((2, steps + 1, 2, 2, 2)),
        dma((2, steps + 1, 2, 2, 2)),
        dma((2, steps + 1, 2, 2, 2)),
        dma((2, n, 2)),
        dma((2, n, 2)),
        dma((2, n, 2, 2)),
        dma((2, 2, 2, steps)),
        dma((2, 2, 2, steps)),
        dma((2, 1)),
        dma((2, 2)),
    ]
    return pl.pallas_call(
        functools.partial(kernel, dims),
        out_shape=jax.ShapeDtypeStruct((rows, cd), BF),
        in_specs=[
            pl.BlockSpec(memory_space=pltpu.HBM if i in (9, 10) else pltpu.VMEM) for i in range(12)
        ],
        out_specs=pl.BlockSpec(memory_space=pltpu.VMEM),
        scratch_shapes=scratch,
        compiler_params=pltpu.CompilerParams(
            collective_id=0, has_side_effects=True, vmem_limit_bytes=62 * 1024 * 1024
        ),
    )(
        tok,
        g1.reshape(1, -1),
        up,
        val,
        vg.reshape(1, -1),
        mw,
        mb,
        back,
        g2.reshape(1, -1),
        hid,
        down,
        g3.reshape(1, -1),
    )


def normalize(values, gain, total, width):
    return values * lax.rsqrt(total / width + EPS) * gain


def on_device(
    tokens,
    first_gain,
    up_weight,
    value_weight,
    value_gain,
    mix_weight,
    mix_bias,
    back_weight,
    mid_gain,
    hidden_weight,
    down_weight,
    last_gain,
):
    col_count = tokens.shape[1]
    row_count = tokens.shape[0]
    width = col_count * lax.axis_size("tp")
    offset = lax.axis_index("tp") * col_count
    inputs = tokens.astype(jnp.float32)
    whole_in = lax.all_gather(tokens, "tp", axis=1, tiled=True).astype(jnp.float32)
    normed = normalize(
        whole_in, first_gain, jnp.sum(whole_in * whole_in, axis=1, keepdims=True), width
    ).astype(jnp.bfloat16)
    gw_dev = up_weight.shape[1]
    block = normed
    up_pre = jnp.dot(
        block,
        lax.all_gather(up_weight, "fs", axis=0, tiled=True),
        preferred_element_type=jnp.float32,
    )
    value_pre = jnp.dot(
        block,
        lax.all_gather(value_weight, "fs", axis=0, tiled=True),
        preferred_element_type=jnp.float32,
    )
    up_part = jax.nn.gelu(up_pre, approximate=False).astype(jnp.bfloat16)
    value_act = jax.nn.gelu(value_pre, approximate=False)
    value_total = lax.psum(jnp.sum(value_act * value_act, axis=1, keepdims=True), "tp")
    value_normed = normalize(
        value_act, value_gain, value_total, gw_dev * lax.axis_size("tp")
    ).astype(jnp.bfloat16)
    group_dev = mix_weight.shape[0]
    span = mix_weight.shape[1]
    causal = jnp.tril(jnp.ones((span, span), dtype=bool))
    masked = jnp.where(causal[None], mix_weight, jnp.zeros_like(mix_weight))
    blocks = value_normed.reshape(row_count // span, span, group_dev, gw_dev // group_dev)
    mixed = (
        jnp.einsum("gts,nsgc->ntgc", masked, blocks, preferred_element_type=jnp.float32)
        + mix_bias.T[None, :, :, None]
    )
    gated = (up_part.astype(jnp.float32) * mixed.reshape(row_count, gw_dev)).astype(jnp.bfloat16)
    gated_all = lax.all_gather(gated, "tp", axis=1, tiled=True)
    block = gated_all
    back = jnp.dot(
        block,
        lax.all_gather(back_weight, "fs", axis=0, tiled=True),
        preferred_element_type=jnp.float32,
    )
    stream = (inputs + back).astype(jnp.bfloat16)
    stream_f = stream.astype(jnp.float32)
    whole_mid = lax.all_gather(stream, "tp", axis=1, tiled=True).astype(jnp.float32)
    mid_normed = normalize(
        whole_mid, mid_gain, jnp.sum(whole_mid * whole_mid, axis=1, keepdims=True), width
    ).astype(jnp.bfloat16)
    block = mid_normed
    hidden_pre = jnp.dot(
        block,
        lax.all_gather(hidden_weight, "fs", axis=0, tiled=True),
        preferred_element_type=jnp.float32,
    )
    hidden = jnp.square(jax.nn.relu(hidden_pre)).astype(jnp.bfloat16)
    partial_terms = jnp.dot(
        hidden,
        lax.all_gather(down_weight, "fs", axis=1, tiled=True),
        preferred_element_type=jnp.float32,
    )
    channel_out = lax.psum_scatter(
        partial_terms.astype(jnp.bfloat16), "tp", scatter_dimension=1, tiled=True
    ).astype(jnp.float32)
    final = stream_f + channel_out
    final_total = lax.psum(jnp.sum(final * final, axis=1, keepdims=True), "tp")
    return normalize(
        final, lax.dynamic_slice_in_dim(last_gain, offset, col_count), final_total, width
    ).astype(jnp.bfloat16)


def fits(mesh, args):
    tok, _, up, _, _, mw, _, back, _, hid, down, _ = args
    n = mesh.shape["fs"]
    rows, cd = tok.shape
    hrows = rows // 2
    fu = hid.shape[1] // n
    if mesh.shape["rep"] != 2 or mesh.shape["tp"] != 2 or n % 2 or n < 4:
        return False
    if hrows % mw.shape[1] or fu % 256 or down.shape[1] % 128 or up.shape[0] % 256 or back.shape[0] % 64:
        return False
    held = 2 * (up.size * 2 + back.size + hid.size + down.size)
    held += 4 * n * (up.size * 2 + back.size) + 4 * (hid.size + down.size)
    held += n * 2 * hrows * cd * 6 + 8 * n * hrows * cd
    return held < 52 * 2**20


def solution(mesh):
    def on_any(*args):
        return fused(mesh, *args) if fits(mesh, args) else on_device(*args)

    return jax.shard_map(
        on_any,
        mesh=mesh,
        in_specs=(
            P(("rep", "fs"), "tp"),
            P(),
            P("fs", "tp"),
            P("fs", "tp"),
            P("tp"),
            P("tp", None, None),
            P("tp", None),
            P("fs", "tp"),
            P(),
            P("fs", "tp"),
            P("tp", "fs"),
            P(),
        ),
        out_specs=P(("rep", "fs"), "tp"),
        check_vma=False,
    )
```
